256 devices in a mesh: fs: 16 (over y, x), tp: 16 (over z, core).
Axes of the slice: x: 4, y: 4, z: 8, core: 2. Of those that a mesh axis runs over, the one named last changes fastest.
Arguments:
- tokens_in: bfloat16 [65536, 2048], P(('fs', 'tp')), may hold values from -6 to 6
- gate_cotangent: bfloat16 [65536, 1024], P(('fs', 'tp')), may hold values from -0.09375 to 0.09375
- conv_output: bfloat16 [65536, 1024], P(('fs', 'tp')), may hold values from -6 to 6
- block_cotangent: bfloat16 [65536, 2048], P(('fs', 'tp')), may hold values from -0.09375 to 0.09375
- projectors: bfloat16 [2048, 2, 256], P('fs'), may hold values from -0.125 to 0.125
- first_moment: float32 [256, 2, 1024], P('fs', None, 'tp'), may hold values from -6 to 6
- second_moment: float32 [256, 2, 1024], P('fs', None, 'tp'), may hold values from 0.25 to 4
- gate_master: float32 [2048, 1024], P('fs', 'tp'), may hold values from -0.125 to 0.125
- out_master: float32 [1024, 2048], P('tp', 'fs'), may hold values from -0.1875 to 0.1875
Outputs:
- first_new: float32 [256, 2, 1024], P('fs', None, 'tp')
- second_new: float32 [256, 2, 1024], P('fs', None, 'tp')
- step_gate: float32 [2048, 1024], P('fs', 'tp')
- step_out: float32 [1024, 2048], P('tp', 'fs')
- gate_new: float32 [2048, 1024], P('fs', 'tp')
- out_new: float32 [1024, 2048], P('tp', 'fs')
- gate_copy: bfloat16 [2048, 1024], P(None, 'tp')
- out_copy: bfloat16 [1024, 2048], P('tp')
The draws below stay inside these ranges and needn't reach their ends.
All inputs are finite; a program needn't handle non-finite values.
Results may differ from the reference program's by a relative error of at most 0.0035.
Values may be sent and summed in bfloat16 or wider, within the bound.
A program may use at most 64 MiB of HBM per device.

```python
import math
import jax
import jax.numpy as jnp
from jax import lax

D = 2048
CH = 1024
RANK = 256
TOKENS = 65536


def raised(result, rng, source, target, parts, factor):
    owner, partner = [(jnp.arange(result.shape[dim]) // (result.shape[dim] // parts)).reshape([-1 if axis == dim else 1 for axis in range(result.ndim)]) for dim in (source, target)]
    chosen = jax.random.permutation(rng, parts)[partner]
    strong = (owner == chosen) | (owner == (partner + parts // 2) % parts)
    return jnp.where(strong, factor * result, result)


def block_scale(own_key, shape, cuts, least, top_value):
    factor_of = 1.0
    for position, shards_of in cuts:
        steps = jax.random.uniform(jax.random.fold_in(jax.random.fold_in(own_key, 6), position), (shards_of,), jnp.float32, least / len(cuts), top_value / len(cuts))
        factor_of = factor_of * jnp.repeat(jnp.exp(steps), shape[position] // shards_of).reshape((-1,) + (1,) * (len(shape) - 1 - position))
    return factor_of


def scatter_about(stream_key, shape, deviation, bound, pieces=(), held_as=jnp.bfloat16):
    entries = jax.random.normal(stream_key, shape, jnp.float32) * deviation
    if len(pieces) > 0:
        entries = block_scale(stream_key, shape, pieces, -0.22, 0.18) * entries
    return jnp.clip(entries, min=-bound, max=bound).astype(held_as)


def heavy_noise(rng, shape, width, reach, pieces, heavy, held_as=jnp.bfloat16):
    result = width * jax.random.normal(rng, shape, jnp.float32)
    if pieces:
        result = result * block_scale(rng, shape, pieces, -0.22, 0.18)
    return jnp.clip(raised(result, jax.random.fold_in(rng, 3), *heavy), -reach, reach).astype(held_as)


def setup_inputs(seed: int = 0) -> dict:
    keys = jax.random.split(jax.random.key(seed), 10)
    return {
        "tokens_in": scatter_about(keys[0], (TOKENS, D), 1.0, 6.0, ((0, 256),)),
        "gate_cotangent": heavy_noise(keys[1], (TOKENS, CH), (TOKENS ** -0.5), 0.09375, ((0, 256),), (0, 1, 256, 6.0)),
        "conv_output": scatter_about(keys[2], (TOKENS, CH), 1.0, 6.0, ((0, 256),)),
        "block_cotangent": heavy_noise(keys[3], (TOKENS, D), (TOKENS ** -0.5), 0.09375, ((0, 256),), (0, 1, 256, 6.0)),
        "projectors": scatter_about(keys[4], (D, 2, RANK), D ** -0.5, 0.125, ((0, 16),)),
        "first_moment": scatter_about(keys[5], (RANK, 2, CH), 1.0, 6.0, ((0, 16), (2, 16)), jnp.float32),
        "second_moment": jnp.clip(jnp.exp(math.log(4.0) - 2.7725887 * jax.random.uniform(keys[6], (RANK, 2, CH), jnp.float32) ** block_scale(keys[6], (RANK, 2, CH), ((0, 16), (2, 16)), -0.2, 0.2)), 0.25, 4.0),
        "gate_master": scatter_about(keys[7], (D, CH), D ** -0.5, 0.125, ((0, 16), (1, 16)), jnp.float32),
        "out_master": scatter_about(keys[8], (CH, D), CH ** -0.5, 0.1875, ((0, 16), (1, 16)), jnp.float32),
    }


def reference(tokens_in, gate_cotangent, conv_output, block_cotangent, projectors, first_moment, second_moment, gate_master, out_master):
    contract_dims = (((0,), (0,)), ((), ()))
    grad_gate = lax.dot_general(tokens_in, gate_cotangent, contract_dims, preferred_element_type=jnp.float32)
    grad_flip = lax.dot_general(block_cotangent, conv_output, contract_dims, preferred_element_type=jnp.float32)
    gradients = jnp.stack((grad_gate, grad_flip), axis=1)
    proj_wide = projectors.astype(jnp.float32)
    low_space = jnp.einsum('dmr,dmc->rmc', proj_wide, gradients, precision=lax.Precision.HIGHEST)
    first_new = 0.8 * first_moment + 0.2 * low_space
    second_new = 0.9 * second_moment + 0.1 * low_space * low_space
    direction = first_new / jnp.sqrt(second_new)
    norm_value = jnp.sqrt(lax.optimization_barrier(jnp.sum(direction * direction, axis=(0, 2))))
    clip_level = 0.5 * math.sqrt(RANK * CH)
    factor = clip_level / jnp.maximum(norm_value, clip_level)
    scaled_step = jnp.einsum('dmr,rmc->dmc', proj_wide, direction, precision=lax.Precision.HIGHEST) * factor[None, :, None]
    step_gate = scaled_step[:, 0, :]
    step_out = scaled_step[:, 1, :].T
    gate_new = gate_master - 0.01 * step_gate
    out_new = out_master - 0.01 * step_out
    return (first_new, second_new, step_gate, step_out, gate_new, out_new, gate_new.astype(jnp.bfloat16), out_new.astype(jnp.bfloat16))
```

```python
import functools
import math

import jax
import jax.numpy as jnp
from jax import lax
from jax.experimental import pallas as pl
from jax.experimental.pallas import tpu as pltpu
from jax.sharding import Mesh
from jax.sharding import PartitionSpec as P

MESH = pl.DeviceIdType.MESH
F32 = jnp.float32
BF16 = jnp.bfloat16
FS = ("y", "x")
TP = ("z", "c")
FS_TP = ("y", "x", "z", "c")

BETA_FIRST = 0.8
BETA_SECOND = 0.9
LEARN_RATE = 0.01
CLIP_SHARE = 0.5


def kernel(
    sizes,
    x_hbm,
    g_hbm,
    cv_hbm,
    b_hbm,
    proj,
    fm,
    sm,
    gm,
    om,
    fn_out,
    sn_out,
    sg_out,
    so_out,
    gn_out,
    on_out,
    gc_out,
    oc_out,
    ax,
    ag,
    pfull,
    mix,
    low,
    lowb,
    rs,
    psf,
    psb,
    zb,
    dall,
    cb,
    ebuf,
    load_sem,
    swap_send,
    swap_recv,
    pf_send,
    pf_recv,
    pa_send,
    pa_recv,
    pb_send,
    pb_recv,
    rs_send,
    rs_recv,
    z_send,
    z_recv,
    d_send,
    d_recv,
    c_send,
    c_recv,
    e_send,
    e_recv,
):
    NY, NX, NZ = sizes
    NFS = NY * NX
    tokens = x_hbm.shape[0]
    rows = proj.shape[0]
    rank = pfull.shape[1]
    rk = rank // NFS
    width = zb.shape[-1]
    half = width // 2
    y, x = lax.axis_index("y"), lax.axis_index("x")
    z, c = lax.axis_index("z"), lax.axis_index("c")
    fs = y * NX + x

    def fs_peer(d):
        return (lax.rem(y + d // NX, NY), lax.rem(x + d % NX, NX), z, c)

    def fs_source(d):
        return lax.rem(y + NY - d // NX, NY) * NX + lax.rem(x + NX - d % NX, NX)

    def tp_peer(e):
        return (y, x, lax.rem(z + e // 2, NZ), lax.rem(c + e % 2, 2))

    partner = (y, x, z, 1 - c)

    def own_loads(act, cot):
        return (
            pltpu.make_async_copy(act, ax.at[0], load_sem.at[0]),
            pltpu.make_async_copy(cot, ag.at[0], load_sem.at[1]),
        )

    def swaps(act, cot):
        return (
            pltpu.make_async_remote_copy(
                act, ax.at[1], swap_send.at[0], swap_recv.at[0], device_id=partner, device_id_type=MESH
            ),
            pltpu.make_async_remote_copy(
                cot, ag.at[1], swap_send.at[1], swap_recv.at[1], device_id=partner, device_id_type=MESH
            ),
        )

    @pl.when(c == 0)
    def _():
        for copy in own_loads(x_hbm, g_hbm):
            copy.start()

    @pl.when(c == 1)
    def _():
        for copy in own_loads(b_hbm, cv_hbm):
            copy.start()

    barrier = pltpu.get_barrier_semaphore()

    @pl.loop(1, NFS)
    def _(d):
        pl.semaphore_signal(barrier, inc=1, device_id=fs_peer(d), device_id_type=MESH)

    @pl.loop(1, 2 * NZ)
    def _(e):
        pl.semaphore_signal(barrier, inc=1, device_id=tp_peer(e), device_id_type=MESH)

    own = pl.multiple_of(fs * rows, rows)
    slab = proj[...]
    pfull[pl.ds(own, rows), :] = jnp.where(c == 0, slab[:, 0, :], slab[:, 1, :])
    pl.semaphore_wait(barrier, NFS - 1 + 2 * NZ - 1)

    def p_copy(src, first, count, send, recv, d, peer):
        at = pl.ds(pl.multiple_of(src * rows + first, count), count)
        return pltpu.make_async_remote_copy(
            pfull.at[at], pfull.at[at], send.at[d], recv.at[d], device_id=peer, device_id_type=MESH
        )

    hr = rows // 2
    axis_offsets = [k for k in range(1, NX)] + [k * NX for k in range(1, NY)]
    for d in axis_offsets:
        p_copy(fs, 0, rows, pf_send, pf_recv, d, fs_peer(d)).start()

    @pl.when(c == 0)
    def _():
        for copy in swaps(b_hbm, cv_hbm):
            copy.start()

    @pl.when(c == 1)
    def _():
        for copy in swaps(x_hbm, g_hbm):
            copy.start()

    for k in range(1, max(NX, NY)):
        if k < NX:
            p_copy(fs_source(k), 0, rows, pf_send, pf_recv, k, fs_peer(k)).wait_recv()
            for j in range(1, NY):
                p_copy(fs_source(k), 0, hr, pa_send, pa_recv, j * NX + k, fs_peer(j * NX)).start()
        if k < NY:
            p_copy(fs_source(k * NX), 0, rows, pf_send, pf_recv, k * NX, fs_peer(k * NX)).wait_recv()
            for j in range(1, NX):
                p_copy(fs_source(k * NX), hr, hr, pb_send, pb_recv, k * NX + j, fs_peer(j)).start()

    for copy in own_loads(x_hbm, g_hbm):
        copy.wait()
    for copy in swaps(x_hbm, g_hbm):
        copy.wait_recv()

    for dy in range(NY):
        if dy > 0:
            for dx in range(1, NX):
                d = dy * NX + dx
                p_copy(fs_source(d), 0, hr, pa_send, pa_recv, d, fs_peer(d)).wait_recv()
                p_copy(fs_source(d), hr, hr, pb_send, pb_recv, d, fs_peer(d)).wait_recv()
        ydim = lax.rem(y + NY - dy, NY)
        at = pl.ds(pl.multiple_of(ydim * (NX * rows), NX * rows), NX * rows)
        for s in range(2):
            term = jnp.dot(ax[s, :, at], pfull[at, :], preferred_element_type=F32)
            span = pl.ds(s * tokens, tokens)
            if dy == 0:
                mix[span, :] = term
            else:
                mix[span, :] += term

    both = mix[...]
    upper = both.astype(BF16)
    lower = (both - upper.astype(F32)).astype(BF16)
    cots = ag[...].reshape(2 * tokens, ag.shape[-1])
    turn = (((0,), (0,)), ((), ()))
    low[...] = lax.dot_general(upper, cots, turn, preferred_element_type=F32) + lax.dot_general(
        lower, cots, turn, preferred_element_type=F32
    )
    lowb[...] = low[...].astype(BF16)

    def rs_copy(d, dst):
        return pltpu.make_async_remote_copy(
            lowb.at[pl.ds(pl.multiple_of(dst * rk, rk), rk)],
            rs.at[d],
            rs_send.at[d],
            rs_recv.at[d],
            device_id=fs_peer(d),
            device_id_type=MESH,
        )

    def fs_target(d):
        return lax.rem(y + d // NX, NY) * NX + lax.rem(x + d % NX, NX)

    for d in range(1, NFS):
        rs_copy(d, fs_target(d)).start()
    total = low[pl.ds(pl.multiple_of(fs * rk, rk), rk), :]
    for d in range(1, NFS):
        rs_copy(d, fs).wait_recv()
        total = total + rs[d].astype(F32)
    psf[...] = total
    psb[...] = total.astype(BF16)

    def z_copy(e):
        zt = lax.rem(z + e // 2, NZ)
        return pltpu.make_async_remote_copy(
            psb.at[:, pl.ds(pl.multiple_of(zt * width, width), width)],
            zb.at[e],
            z_send.at[e],
            z_recv.at[e],
            device_id=tp_peer(e),
            device_id_type=MESH,
        )

    for e in range(1, 2 * NZ):
        z_copy(e).start()
    same = psf[:, pl.ds(pl.multiple_of(z * width, width), width)]
    other = jnp.zeros_like(same)
    for e in range(1, 2 * NZ):
        z_copy(e).wait_recv()
        if e % 2:
            other = other + zb[e].astype(F32)
        else:
            same = same + zb[e].astype(F32)

    fm_in, sm_in = fm[...], sm[...]
    directions = []
    for m in range(2):
        whole = jnp.where(c == m, same, other)
        part = jnp.where(c == 0, whole[:, :half], whole[:, half:])
        first = BETA_FIRST * fm_in[:, m, :] + (1.0 - BETA_FIRST) * part
        second = BETA_SECOND * sm_in[:, m, :] + (1.0 - BETA_SECOND) * part * part
        fn_out[:, m, :] = first
        sn_out[:, m, :] = second
        directions.append(first / jnp.sqrt(second))
    mine = pl.ds(pl.multiple_of(fs * rk, rk), rk)
    dall[mine, :] = jnp.concatenate(directions, axis=1).astype(BF16)

    def d_copy(d, src):
        at = pl.ds(pl.multiple_of(src * rk, rk), rk)
        return pltpu.make_async_remote_copy(
            dall.at[at], dall.at[at], d_send.at[d], d_recv.at[d], device_id=fs_peer(d), device_id_type=MESH
        )

    for d in range(1, NFS):
        d_copy(d, fs).start()
    for d in range(1, NFS):
        d_copy(d, fs_source(d)).wait_recv()

    rotated = dall[...]
    wide = rotated.astype(F32)
    cb[0] = jnp.sum((wide * wide).reshape(rank // 8, 8, width), axis=0)

    def c_copy(e):
        return pltpu.make_async_remote_copy(
            cb.at[0], cb.at[e], c_send.at[e], c_recv.at[e], device_id=tp_peer(e), device_id_type=MESH
        )

    for e in range(1, 2 * NZ):
        c_copy(e).start()

    raws = []
    for m in range(2):
        raw = lax.dot_general(rotated, slab[:, m, :], (((0,), (1,)), ((), ())), preferred_element_type=F32)
        raws.append(raw[m * half : (m + 1) * half])

    squares = cb[0]
    for e in range(1, 2 * NZ):
        c_copy(e).wait_recv()
        squares = squares + cb[e]
    clip_level = CLIP_SHARE * math.sqrt(rank * width * NZ)
    masters = (gm, om)
    steps = (sg_out, so_out)
    news = (gn_out, on_out)
    for m in range(2):
        norm = jnp.sqrt(jnp.sum(squares[:, m * half : (m + 1) * half], axis=(0, 1), keepdims=True))
        factor = clip_level / jnp.maximum(norm, clip_level)
        step = raws[m] * factor
        new = masters[m][...] - LEARN_RATE * step
        steps[m][...] = step
        news[m][...] = new
        ebuf[m, :, pl.ds(own, rows)] = new.astype(BF16)

    def e_copy(d, src):
        at = pl.ds(pl.multiple_of(src * rows, rows), rows)
        return pltpu.make_async_remote_copy(
            ebuf.at[:, :, at], ebuf.at[:, :, at], e_send.at[d], e_recv.at[d], device_id=fs_peer(d), device_id_type=MESH
        )

    for d in range(1, NFS):
        e_copy(d, fs).start()
    for d in range(1, NFS):
        e_copy(d, fs_source(d)).wait_recv()
    gc_out[...] = ebuf[0]
    oc_out[...] = ebuf[1]

    for d in axis_offsets:
        p_copy(fs, 0, rows, pf_send, pf_recv, d, fs_peer(d)).wait_send()
    for d in range(1, NFS):
        if d // NX and d % NX:
            p_copy(fs, 0, hr, pa_send, pa_recv, d, fs_peer(d)).wait_send()
            p_copy(fs, hr, hr, pb_send, pb_recv, d, fs_peer(d)).wait_send()
        rs_copy(d, fs).wait_send()
        d_copy(d, fs).wait_send()
        e_copy(d, fs).wait_send()
    for e in range(1, 2 * NZ):
        z_copy(e).wait_send()
        c_copy(e).wait_send()
    for copy in swaps(x_hbm, g_hbm):
        copy.wait_send()


def shards(sizes, x, g, cv, b, proj, fm, sm, gm, om):
    NY, NX, NZ = sizes
    NFS = NY * NX
    tokens, d_model = x.shape
    channels = g.shape[1]
    rows, _, rank = proj.shape
    rk = rank // NFS
    cols = gm.shape[1]
    width = 2 * cols
    vmem = pl.BlockSpec(memory_space=pltpu.VMEM)
    hbm = pl.BlockSpec(memory_space=pl.ANY)
    dma = pltpu.SemaphoreType.DMA
    small = jax.ShapeDtypeStruct(fm.shape, F32)
    block = jax.ShapeDtypeStruct((cols, rows), F32)
    copy = jax.ShapeDtypeStruct((cols, d_model), BF16)
    fn, sn, sg, so, gn, on, gc, oc = pl.pallas_call(
        functools.partial(kernel, sizes),
        out_shape=(small, small, block, block, block, block, copy, copy),
        in_specs=[hbm] * 4 + [vmem] * 5,
        out_specs=(vmem,) * 8,
        scratch_shapes=[
            pltpu.VMEM((2, tokens, d_model), BF16),
            pltpu.VMEM((2, tokens, channels), BF16),
            pltpu.VMEM((d_model, rank), BF16),
            pltpu.VMEM((2 * tokens, rank), F32),
            pltpu.VMEM((rank, channels), F32),
            pltpu.VMEM((rank, channels), BF16),
            pltpu.VMEM((NFS, rk, channels), BF16),
            pltpu.VMEM((rk, channels), F32),
            pltpu.VMEM((rk, channels), BF16),
            pltpu.VMEM((2 * NZ, rk, width), BF16),
            pltpu.VMEM((rank, width), BF16),
            pltpu.VMEM((2 * NZ, 8, width), F32),
            pltpu.VMEM((2, cols, d_model), BF16),
            dma((2,)),
            dma((2,)),
            dma((2,)),
        ]
        + [dma((NFS,))] * 8
        + [dma((2 * NZ,))] * 2
        + [dma((NFS,))] * 2
        + [dma((2 * NZ,))] * 2
        + [dma((NFS,))] * 2,
        compiler_params=pltpu.CompilerParams(collective_id=0, has_side_effects=True, vmem_limit_bytes=48 * 2**20),
    )(x, g, cv, b, proj, fm, sm, gm.T, om)
    return fn, sn, sg.T, so, gn.T, on, gc.T, oc


def solution(mesh):
    sizes = (4, 4, 8)
    split = Mesh(mesh.devices.reshape(*sizes, 2), FS_TP)
    return build(split, sizes)


def build(split, sizes):
    in_specs = (
        P(FS_TP, None),
        P(FS_TP, None),
        P(FS_TP, None),
        P(FS_TP, None),
        P(FS, None, None),
        P(FS, None, TP),
        P(FS, None, TP),
        P(FS, TP),
        P(TP, FS),
    )
    out_specs = (
        P(FS, None, TP),
        P(FS, None, TP),
        P(FS, TP),
        P(TP, FS),
        P(FS, TP),
        P(TP, FS),
        P(None, TP),
        P(TP, None),
    )
    return jax.shard_map(
        functools.partial(shards, sizes), mesh=split, in_specs=in_specs, out_specs=out_specs, check_vma=False
    )
```

```python
import functools
import math

import jax
import jax.numpy as jnp
from jax import lax
from jax.experimental import pallas as pl
from jax.experimental.pallas import tpu as pltpu
from jax.sharding import Mesh
from jax.sharding import PartitionSpec as P

MESH = pl.DeviceIdType.MESH
F32 = jnp.float32
BF16 = jnp.bfloat16
FS = ("y", "x")
TP = ("z", "c")
FS_TP = ("y", "x", "z", "c")

BETA_FIRST = 0.8
BETA_SECOND = 0.9
LEARN_RATE = 0.01
CLIP_SHARE = 0.5


def kernel(
    sizes,
    x_hbm,
    g_hbm,
    cv_hbm,
    b_hbm,
    proj_hbm,
    fm_hbm,
    sm_hbm,
    gm_hbm,
    om_hbm,
    fn_out,
    sn_out,
    sg_out,
    so_out,
    gn_out,
    on_out,
    ebuf,
    proj,
    fm,
    sm,
    ax,
    ag,
    pboth,
    masters,
    raws,
    mix,
    low,
    lowb,
    rs,
    psf,
    psb,
    zb,
    dall,
    cb,
    load_sem,
    swap_send,
    swap_recv,
    pf_send,
    pf_recv,
    pa_send,
    pa_recv,
    pb_send,
    pb_recv,
    rs_send,
    rs_recv,
    z_send,
    z_recv,
    d_send,
    d_recv,
    c_send,
    c_recv,
    po_sem,
    mf_send,
    mf_recv,
    md_send,
    md_recv,
):
    NY, NX, NZ = sizes
    NFS = NY * NX
    tokens = x_hbm.shape[0]
    rows = proj.shape[0]
    rank = pboth.shape[2]
    rk = rank // NFS
    width = zb.shape[-1]
    half = width // 2
    y, x = lax.axis_index("y"), lax.axis_index("x")
    z, c = lax.axis_index("z"), lax.axis_index("c")
    fs = y * NX + x
    pfull = pboth.at[c]
    own = pl.multiple_of(fs * rows, rows)
    own_lanes = pl.ds(own, rows)

    def fs_peer(d):
        return (lax.rem(y + d // NX, NY), lax.rem(x + d % NX, NX), z, c)

    def fs_source(d):
        return lax.rem(y + NY - d // NX, NY) * NX + lax.rem(x + NX - d % NX, NX)

    def tp_peer(e):
        return (y, x, lax.rem(z + e // 2, NZ), lax.rem(c + e % 2, 2))

    partner = (y, x, z, 1 - c)

    def own_loads(act, cot):
        return (
            pltpu.make_async_copy(act, ax.at[0], load_sem.at[0]),
            pltpu.make_async_copy(cot, ag.at[0], load_sem.at[1]),
        )

    def swaps(act, cot):
        return (
            pltpu.make_async_remote_copy(
                act, ax.at[1], swap_send.at[0], swap_recv.at[0], device_id=partner, device_id_type=MESH
            ),
            pltpu.make_async_remote_copy(
                cot, ag.at[1], swap_send.at[1], swap_recv.at[1], device_id=partner, device_id_type=MESH
            ),
        )

    proj_load = pltpu.make_async_copy(proj_hbm, proj, load_sem.at[2])
    proj_load.start()

    @pl.when(c == 0)
    def _():
        for copy in own_loads(x_hbm, g_hbm):
            copy.start()

    @pl.when(c == 1)
    def _():
        for copy in own_loads(b_hbm, cv_hbm):
            copy.start()

    late_loads = [
        pltpu.make_async_copy(src, dst, load_sem.at[3 + i])
        for i, (src, dst) in enumerate(
            ((fm_hbm, fm), (sm_hbm, sm), (gm_hbm, masters.at[0, :, own_lanes]), (om_hbm, masters.at[1, :, own_lanes]))
        )
    ]
    for copy in late_loads:
        copy.start()

    barrier = pltpu.get_barrier_semaphore()

    @pl.loop(1, NFS)
    def _(d):
        pl.semaphore_signal(barrier, inc=1, device_id=fs_peer(d), device_id_type=MESH)

    @pl.loop(1, 2 * NZ)
    def _(e):
        pl.semaphore_signal(barrier, inc=1, device_id=tp_peer(e), device_id_type=MESH)

    proj_load.wait()
    slab = proj[...]
    pfull[pl.ds(own, rows), :] = jnp.where(c == 0, slab[:, 0, :], slab[:, 1, :])
    pl.semaphore_wait(barrier, NFS - 1 + 2 * NZ - 1)

    def p_copy(src, first, count, send, recv, d, peer):
        at = pl.ds(pl.multiple_of(src * rows + first, count), count)
        return pltpu.make_async_remote_copy(
            pfull.at[at], pfull.at[at], send.at[d], recv.at[d], device_id=peer, device_id_type=MESH
        )

    hr = rows // 2
    axis_offsets = [k for k in range(1, NX)] + [k * NX for k in range(1, NY)]
    for d in axis_offsets:
        p_copy(fs, 0, rows, pf_send, pf_recv, d, fs_peer(d)).start()

    @pl.when(c == 0)
    def _():
        for copy in swaps(b_hbm, cv_hbm):
            copy.start()

    @pl.when(c == 1)
    def _():
        for copy in swaps(x_hbm, g_hbm):
            copy.start()

    for k in range(1, max(NX, NY)):
        if k < NX:
            p_copy(fs_source(k), 0, rows, pf_send, pf_recv, k, fs_peer(k)).wait_recv()
            for j in range(1, NY):
                p_copy(fs_source(k), 0, hr, pa_send, pa_recv, j * NX + k, fs_peer(j * NX)).start()
        if k < NY:
            p_copy(fs_source(k * NX), 0, rows, pf_send, pf_recv, k * NX, fs_peer(k * NX)).wait_recv()
            for j in range(1, NX):
                p_copy(fs_source(k * NX), hr, hr, pb_send, pb_recv, k * NX + j, fs_peer(j)).start()

    for copy in own_loads(x_hbm, g_hbm):
        copy.wait()
    for copy in swaps(x_hbm, g_hbm):
        copy.wait_recv()

    for dy in range(NY):
        if dy > 0:
            for dx in range(1, NX):
                d = dy * NX + dx
                p_copy(fs_source(d), 0, hr, pa_send, pa_recv, d, fs_peer(d)).wait_recv()
                p_copy(fs_source(d), hr, hr, pb_send, pb_recv, d, fs_peer(d)).wait_recv()
        ydim = lax.rem(y + NY - dy, NY)
        at = pl.ds(pl.multiple_of(ydim * (NX * rows), NX * rows), NX * rows)
        for s in range(2):
            term = jnp.dot(ax[s, :, at], pfull[at, :], preferred_element_type=F32)
            span = pl.ds(s * tokens, tokens)
            if dy == 0:
                mix[span, :] = term
            else:
                mix[span, :] += term

    both = mix[...]
    upper = both.astype(BF16)
    lower = (both - upper.astype(F32)).astype(BF16)
    cots = ag[...].reshape(2 * tokens, ag.shape[-1])
    turn = (((0,), (0,)), ((), ()))
    low[...] = lax.dot_general(upper, cots, turn, preferred_element_type=F32) + lax.dot_general(
        lower, cots, turn, preferred_element_type=F32
    )
    lowb[...] = low[...].astype(BF16)

    po_copy = pltpu.make_async_remote_copy(
        pfull, pfull, po_sem.at[0], po_sem.at[1], device_id=partner, device_id_type=MESH
    )
    po_copy.start()

    def rs_copy(d, dst):
        return pltpu.make_async_remote_copy(
            lowb.at[pl.ds(pl.multiple_of(dst * rk, rk), rk)],
            rs.at[d],
            rs_send.at[d],
            rs_recv.at[d],
            device_id=fs_peer(d),
            device_id_type=MESH,
        )

    def fs_target(d):
        return lax.rem(y + d // NX, NY) * NX + lax.rem(x + d % NX, NX)

    for d in range(1, NFS):
        rs_copy(d, fs_target(d)).start()
    total = low[pl.ds(pl.multiple_of(fs * rk, rk), rk), :]
    for d in range(1, NFS):
        rs_copy(d, fs).wait_recv()
        total = total + rs[d].astype(F32)
    psf[...] = total
    psb[...] = total.astype(BF16)

    def z_copy(e):
        zt = lax.rem(z + e // 2, NZ)
        return pltpu.make_async_remote_copy(
            psb.at[:, pl.ds(pl.multiple_of(zt * width, width), width)],
            zb.at[e],
            z_send.at[e],
            z_recv.at[e],
            device_id=tp_peer(e),
            device_id_type=MESH,
        )

    for e in range(1, 2 * NZ):
        z_copy(e).start()

    for copy in late_loads:
        copy.wait()

    def m_copy(m, src, send, recv, d, peer):
        at = pl.ds(pl.multiple_of(src * rows, rows), rows)
        return pltpu.make_async_remote_copy(
            masters.at[m, :, at], masters.at[m, :, at], send.at[m, d], recv.at[m, d], device_id=peer, device_id_type=MESH
        )

    for d in axis_offsets:
        for m in range(2):
            m_copy(m, fs, mf_send, mf_recv, d, fs_peer(d)).start()

    same = psf[:, pl.ds(pl.multiple_of(z * width, width), width)]
    other = jnp.zeros_like(same)
    for e in range(1, 2 * NZ):
        z_copy(e).wait_recv()
        if e % 2:
            other = other + zb[e].astype(F32)
        else:
            same = same + zb[e].astype(F32)

    fm_in, sm_in = fm[...], sm[...]
    directions = []
    for m in range(2):
        whole = jnp.where(c == m, same, other)
        part = jnp.where(c == 0, whole[:, :half], whole[:, half:])
        first = BETA_FIRST * fm_in[:, m, :] + (1.0 - BETA_FIRST) * part
        second = BETA_SECOND * sm_in[:, m, :] + (1.0 - BETA_SECOND) * part * part
        fn_out[:, m, :] = first
        sn_out[:, m, :] = second
        directions.append(first / jnp.sqrt(second))
    mine = pl.ds(pl.multiple_of(fs * rk, rk), rk)
    dall[mine, :] = jnp.concatenate(directions, axis=1).astype(BF16)

    def d_copy(d, src):
        at = pl.ds(pl.multiple_of(src * rk, rk), rk)
        return pltpu.make_async_remote_copy(
            dall.at[at], dall.at[at], d_send.at[d], d_recv.at[d], device_id=fs_peer(d), device_id_type=MESH
        )

    for d in range(1, NFS):
        d_copy(d, fs).start()
    for d in range(1, NFS):
        d_copy(d, fs_source(d)).wait_recv()

    rotated = dall[...]
    wide = rotated.astype(F32)
    cb[0] = jnp.sum((wide * wide).reshape(rank // 8, 8, width), axis=0)

    def c_copy(e):
        return pltpu.make_async_remote_copy(
            cb.at[0], cb.at[e], c_send.at[e], c_recv.at[e], device_id=tp_peer(e), device_id_type=MESH
        )

    for e in range(1, 2 * NZ):
        c_copy(e).start()

    for k in range(1, NX):
        for m in range(2):
            m_copy(m, fs_source(k), mf_send, mf_recv, k, fs_peer(k)).wait_recv()
        for j in range(1, NY):
            m_copy(0, fs_source(k), md_send, md_recv, j * NX + k, fs_peer(j * NX)).start()
    for k in range(1, NY):
        for m in range(2):
            m_copy(m, fs_source(k * NX), mf_send, mf_recv, k * NX, fs_peer(k * NX)).wait_recv()
        for j in range(1, NX):
            m_copy(1, fs_source(k * NX), md_send, md_recv, k * NX + j, fs_peer(j)).start()

    po_copy.wait_recv()
    turned = rotated.T
    for m in range(2):
        raws[m] = lax.dot_general(
            turned[m * half : (m + 1) * half], pboth[m], (((1,), (1,)), ((), ())), preferred_element_type=F32
        )

    squares = cb[0]
    for e in range(1, 2 * NZ):
        c_copy(e).wait_recv()
        squares = squares + cb[e]
    clip_level = CLIP_SHARE * math.sqrt(rank * width * NZ)
    factors = []
    for m in range(2):
        norm = jnp.sqrt(jnp.sum(squares[:, m * half : (m + 1) * half], axis=(0, 1), keepdims=True))
        factors.append(clip_level / jnp.maximum(norm, clip_level))
    steps = (sg_out, so_out)
    news = (gn_out, on_out)
    for m in range(2):
        step = raws[m, :, own_lanes] * factors[m]
        steps[m][...] = step
        news[m][...] = masters[m, :, own_lanes] - LEARN_RATE * step
    for d in range(1, NFS):
        if d // NX and d % NX:
            for m in range(2):
                m_copy(m, fs_source(d), md_send, md_recv, d, fs_peer(d)).wait_recv()
    for m in range(2):
        ebuf[m] = (masters[m] - LEARN_RATE * (raws[m] * factors[m])).astype(BF16)

    for d in axis_offsets:
        p_copy(fs, 0, rows, pf_send, pf_recv, d, fs_peer(d)).wait_send()
        for m in range(2):
            m_copy(m, fs, mf_send, mf_recv, d, fs_peer(d)).wait_send()
    po_copy.wait_send()
    for d in range(1, NFS):
        if d // NX and d % NX:
            p_copy(fs, 0, hr, pa_send, pa_recv, d, fs_peer(d)).wait_send()
            p_copy(fs, hr, hr, pb_send, pb_recv, d, fs_peer(d)).wait_send()
            for m in range(2):
                m_copy(m, fs, md_send, md_recv, d, fs_peer(d)).wait_send()
        rs_copy(d, fs).wait_send()
        d_copy(d, fs).wait_send()
    for e in range(1, 2 * NZ):
        z_copy(e).wait_send()
        c_copy(e).wait_send()
    for copy in swaps(x_hbm, g_hbm):
        copy.wait_send()


def store_kernel(*refs):
    count = (len(refs) - 2) // 2
    ins, outs, sem = refs[:count], refs[count:-1], refs[-1]
    sources = [*ins[:-1], ins[-1].at[0], ins[-1].at[1]]
    copies = [pltpu.make_async_copy(src, dst, sem.at[i]) for i, (src, dst) in enumerate(zip(sources, outs))]
    for copy in copies:
        copy.start()
    for copy in copies:
        copy.wait()


def shards(sizes, x, g, cv, b, proj, fm, sm, gm, om):
    NY, NX, NZ = sizes
    NFS = NY * NX
    tokens, d_model = x.shape
    channels = g.shape[1]
    rows, _, rank = proj.shape
    rk = rank // NFS
    cols = gm.shape[1]
    width = 2 * cols
    vmem = pl.BlockSpec(memory_space=pltpu.VMEM)
    hbm = pl.BlockSpec(memory_space=pltpu.HBM)
    dma = pltpu.SemaphoreType.DMA
    small = jax.ShapeDtypeStruct(fm.shape, F32)
    block = jax.ShapeDtypeStruct((cols, rows), F32)
    copy = jax.ShapeDtypeStruct((cols, d_model), BF16)
    results = pl.pallas_call(
        functools.partial(kernel, sizes),
        out_shape=(small, small, block, block, block, block, jax.ShapeDtypeStruct((2, cols, d_model), BF16)),
        in_specs=[hbm] * 9,
        out_specs=(vmem,) * 7,
        scratch_shapes=[
            pltpu.VMEM(proj.shape, BF16),
            pltpu.VMEM(fm.shape, F32),
            pltpu.VMEM(sm.shape, F32),
            pltpu.VMEM((2, tokens, d_model), BF16),
            pltpu.VMEM((2, tokens, channels), BF16),
            pltpu.VMEM((2, d_model, rank), BF16),
            pltpu.VMEM((2, cols, d_model), F32),
            pltpu.VMEM((2, cols, d_model), F32),
            pltpu.VMEM((2 * tokens, rank), F32),
            pltpu.VMEM((rank, channels), F32),
            pltpu.VMEM((rank, channels), BF16),
            pltpu.VMEM((NFS, rk, channels), BF16),
            pltpu.VMEM((rk, channels), F32),
            pltpu.VMEM((rk, channels), BF16),
            pltpu.VMEM((2 * NZ, rk, width), BF16),
            pltpu.VMEM((rank, width), BF16),
            pltpu.VMEM((2 * NZ, 8, width), F32),
            dma((7,)),
            dma((2,)),
            dma((2,)),
        ]
        + [dma((NFS,))] * 8
        + [dma((2 * NZ,))] * 2
        + [dma((NFS,))] * 2
        + [dma((2 * NZ,))] * 2
        + [dma((2,))]
        + [dma((2, NFS))] * 4,
        compiler_params=pltpu.CompilerParams(collective_id=0, has_side_effects=True, vmem_limit_bytes=48 * 2**20),
    )(*(pltpu.with_memory_space_constraint(a, pltpu.HBM) for a in (x, g, cv, b, proj, fm, sm, gm.T, om)))
    fn, sn, sg, so, gn, on, gc, oc = pl.pallas_call(
        store_kernel,
        out_shape=(small, small, block, block, block, block, copy, copy),
        in_specs=[vmem] * 7,
        out_specs=(hbm,) * 8,
        scratch_shapes=[dma((8,))],
        compiler_params=pltpu.CompilerParams(vmem_limit_bytes=2**20),
    )(*results)
    return fn, sn, sg.T, so, gn.T, on, gc.T, oc


def solution(mesh):
    sizes = (4, 4, 8)
    split = Mesh(mesh.devices.reshape(*sizes, 2), FS_TP)
    return build(split, sizes)


def build(split, sizes):
    in_specs = (
        P(FS_TP, None),
        P(FS_TP, None),
        P(FS_TP, None),
        P(FS_TP, None),
        P(FS, None, None),
        P(FS, None, TP),
        P(FS, None, TP),
        P(FS, TP),
        P(TP, FS),
    )
    out_specs = (
        P(FS, None, TP),
        P(FS, None, TP),
        P(FS, TP),
        P(TP, FS),
        P(FS, TP),
        P(TP, FS),
        P(None, TP),
        P(TP, None),
    )
    return jax.shard_map(
        functools.partial(shards, sizes), mesh=split, in_specs=in_specs, out_specs=out_specs, check_vma=False
    )
```

```python
import functools
import math

import jax
import jax.numpy as jnp
from jax import lax
from jax.experimental import pallas as pl
from jax.experimental.pallas import tpu as pltpu
from jax.sharding import Mesh
from jax.sharding import PartitionSpec as P

MESH = pl.DeviceIdType.MESH
F32 = jnp.float32
BF16 = jnp.bfloat16
FS = ("y", "x")
TP = ("z", "c")
FS_TP = ("y", "x", "z", "c")

BETA_FIRST = 0.8
BETA_SECOND = 0.9
LEARN_RATE = 0.01
CLIP_SHARE = 0.5


def kernel(
    sizes,
    x_hbm,
    g_hbm,
    cv_hbm,
    b_hbm,
    proj_hbm,
    fm_hbm,
    sm_hbm,
    gm_hbm,
    om_hbm,
    fn_out,
    sn_out,
    sg_out,
    so_out,
    gn_out,
    on_out,
    ebuf,
    proj,
    fm,
    sm,
    ax,
    ag,
    pboth,
    masters,
    raws,
    mix,
    low,
    lowb,
    rs,
    psf,
    psb,
    zb,
    dall,
    cb,
    load_sem,
    swap_send,
    swap_recv,
    pf_send,
    pf_recv,
    pa_send,
    pa_recv,
    pb_send,
    pb_recv,
    rs_send,
    rs_recv,
    z_send,
    z_recv,
    d_send,
    d_recv,
    c_send,
    c_recv,
    po_sem,
    mf_send,
    mf_recv,
    md_send,
    md_recv,
    line_sem,
):
    NY, NX, NZ = sizes
    NFS = NY * NX
    tokens = x_hbm.shape[0]
    rows = proj.shape[0]
    rank = pboth.shape[2]
    rk = rank // NFS
    width = zb.shape[-1]
    half = width // 2
    y, x = lax.axis_index("y"), lax.axis_index("x")
    z, c = lax.axis_index("z"), lax.axis_index("c")
    fs = y * NX + x
    pfull = pboth.at[c]
    own = pl.multiple_of(fs * rows, rows)
    own_lanes = pl.ds(own, rows)

    def fs_peer(d):
        return (lax.rem(y + d // NX, NY), lax.rem(x + d % NX, NX), z, c)

    def fs_source(d):
        return lax.rem(y + NY - d // NX, NY) * NX + lax.rem(x + NX - d % NX, NX)

    def tp_peer(e):
        return (y, x, lax.rem(z + e // 2, NZ), lax.rem(c + e % 2, 2))

    partner = (y, x, z, 1 - c)

    def own_loads(act, cot):
        return (
            pltpu.make_async_copy(act, ax.at[0], load_sem.at[0]),
            pltpu.make_async_copy(cot, ag.at[0], load_sem.at[1]),
        )

    def swaps(act, cot):
        return (
            pltpu.make_async_remote_copy(
                act, ax.at[1], swap_send.at[0], swap_recv.at[0], device_id=partner, device_id_type=MESH
            ),
            pltpu.make_async_remote_copy(
                cot, ag.at[1], swap_send.at[1], swap_recv.at[1], device_id=partner, device_id_type=MESH
            ),
        )

    proj_load = pltpu.make_async_copy(proj_hbm, proj, load_sem.at[2])
    proj_load.start()
    axis_offsets = [k for k in range(1, NX)] + [k * NX for k in range(1, NY)]
    z_neighbours = ((y, x, lax.rem(z + 1, NZ), c), (y, x, lax.rem(z + NZ - 1, NZ), c))
    greeted = [fs_peer(d) for d in axis_offsets] + [partner, *z_neighbours]
    barrier = pltpu.get_barrier_semaphore()
    for peer in greeted:
        pl.semaphore_signal(barrier, inc=1, device_id=peer, device_id_type=MESH)

    @pl.when(c == 0)
    def _():
        for copy in own_loads(x_hbm, g_hbm):
            copy.start()

    @pl.when(c == 1)
    def _():
        for copy in own_loads(b_hbm, cv_hbm):
            copy.start()

    late_loads = [
        pltpu.make_async_copy(src, dst, load_sem.at[3 + i])
        for i, (src, dst) in enumerate(
            ((fm_hbm, fm), (sm_hbm, sm), (gm_hbm, masters.at[0, :, own_lanes]), (om_hbm, masters.at[1, :, own_lanes]))
        )
    ]
    for copy in late_loads:
        copy.start()

    def line_signal(r):
        for peer in z_neighbours:
            pl.semaphore_signal(line_sem.at[r], inc=1, device_id=peer, device_id_type=MESH)

    def line_wait(r):
        pl.semaphore_wait(line_sem.at[r], 2)

    proj_load.wait()
    slab = proj[...]
    pfull[pl.ds(own, rows), :] = jnp.where(c == 0, slab[:, 0, :], slab[:, 1, :])
    pl.semaphore_wait(barrier, len(greeted))
    line_signal(0)

    def p_copy(src, first, count, send, recv, d, peer):
        at = pl.ds(pl.multiple_of(src * rows + first, count), count)
        return pltpu.make_async_remote_copy(
            pfull.at[at], pfull.at[at], send.at[d], recv.at[d], device_id=peer, device_id_type=MESH
        )

    hr = rows // 2
    for d in axis_offsets:
        p_copy(fs, 0, rows, pf_send, pf_recv, d, fs_peer(d)).start()

    @pl.when(c == 0)
    def _():
        for copy in swaps(b_hbm, cv_hbm):
            copy.start()

    @pl.when(c == 1)
    def _():
        for copy in swaps(x_hbm, g_hbm):
            copy.start()

    for k in range(1, max(NX, NY)):
        if k < NX:
            p_copy(fs_source(k), 0, rows, pf_send, pf_recv, k, fs_peer(k)).wait_recv()
            for j in range(1, NY):
                p_copy(fs_source(k), 0, hr, pa_send, pa_recv, j * NX + k, fs_peer(j * NX)).start()
        if k < NY:
            p_copy(fs_source(k * NX), 0, rows, pf_send, pf_recv, k * NX, fs_peer(k * NX)).wait_recv()
            for j in range(1, NX):
                p_copy(fs_source(k * NX), hr, hr, pb_send, pb_recv, k * NX + j, fs_peer(j)).start()

    line_wait(0)
    line_signal(1)

    for copy in own_loads(x_hbm, g_hbm):
        copy.wait()
    for copy in swaps(x_hbm, g_hbm):
        copy.wait_recv()

    for dy in range(NY):
        if dy > 0:
            for dx in range(1, NX):
                d = dy * NX + dx
                p_copy(fs_source(d), 0, hr, pa_send, pa_recv, d, fs_peer(d)).wait_recv()
                p_copy(fs_source(d), hr, hr, pb_send, pb_recv, d, fs_peer(d)).wait_recv()
        ydim = lax.rem(y + NY - dy, NY)
        at = pl.ds(pl.multiple_of(ydim * (NX * rows), NX * rows), NX * rows)
        for s in range(2):
            term = jnp.dot(ax[s, :, at], pfull[at, :], preferred_element_type=F32)
            span = pl.ds(s * tokens, tokens)
            if dy == 0:
                mix[span, :] = term
            else:
                mix[span, :] += term

    line_wait(1)
    line_signal(2)

    both = mix[...]
    upper = both.astype(BF16)
    lower = (both - upper.astype(F32)).astype(BF16)
    cots = ag[...].reshape(2 * tokens, ag.shape[-1])
    turn = (((0,), (0,)), ((), ()))
    low[...] = lax.dot_general(upper, cots, turn, preferred_element_type=F32) + lax.dot_general(
        lower, cots, turn, preferred_element_type=F32
    )
    lowb[...] = low[...].astype(BF16)

    po_copy = pltpu.make_async_remote_copy(
        pfull, pfull, po_sem.at[0], po_sem.at[1], device_id=partner, device_id_type=MESH
    )
    po_copy.start()

    def rs_copy(d, dst):
        return pltpu.make_async_remote_copy(
            lowb.at[pl.ds(pl.multiple_of(dst * rk, rk), rk)],
            rs.at[d],
            rs_send.at[d],
            rs_recv.at[d],
            device_id=fs_peer(d),
            device_id_type=MESH,
        )

    def fs_target(d):
        return lax.rem(y + d // NX, NY) * NX + lax.rem(x + d % NX, NX)

    for d in range(1, NFS):
        rs_copy(d, fs_target(d)).start()
    line_wait(2)
    line_signal(3)
    total = low[pl.ds(pl.multiple_of(fs * rk, rk), rk), :]
    for d in range(1, NFS):
        rs_copy(d, fs).wait_recv()
        total = total + rs[d].astype(F32)
    psf[...] = total
    psb[...] = total.astype(BF16)

    def z_copy(e):
        zt = lax.rem(z + e // 2, NZ)
        return pltpu.make_async_remote_copy(
            psb.at[:, pl.ds(pl.multiple_of(zt * width, width), width)],
            zb.at[e],
            z_send.at[e],
            z_recv.at[e],
            device_id=tp_peer(e),
            device_id_type=MESH,
        )

    line_wait(3)
    for e in range(1, 2 * NZ):
        z_copy(e).start()

    for copy in late_loads:
        copy.wait()

    def m_copy(m, src, send, recv, d, peer):
        at = pl.ds(pl.multiple_of(src * rows, rows), rows)
        return pltpu.make_async_remote_copy(
            masters.at[m, :, at], masters.at[m, :, at], send.at[m, d], recv.at[m, d], device_id=peer, device_id_type=MESH
        )

    for d in axis_offsets:
        for m in range(2):
            m_copy(m, fs, mf_send, mf_recv, d, fs_peer(d)).start()

    same = psf[:, pl.ds(pl.multiple_of(z * width, width), width)]
    other = jnp.zeros_like(same)
    for e in range(1, 2 * NZ):
        z_copy(e).wait_recv()
        if e % 2:
            other = other + zb[e].astype(F32)
        else:
            same = same + zb[e].astype(F32)

    fm_in, sm_in = fm[...], sm[...]
    directions = []
    for m in range(2):
        whole = jnp.where(c == m, same, other)
        part = jnp.where(c == 0, whole[:, :half], whole[:, half:])
        first = BETA_FIRST * fm_in[:, m, :] + (1.0 - BETA_FIRST) * part
        second = BETA_SECOND * sm_in[:, m, :] + (1.0 - BETA_SECOND) * part * part
        fn_out[:, m, :] = first
        sn_out[:, m, :] = second
        directions.append(first / jnp.sqrt(second))
    mine = pl.ds(pl.multiple_of(fs * rk, rk), rk)
    dall[mine, :] = jnp.concatenate(directions, axis=1).astype(BF16)

    def d_copy(d, src):
        at = pl.ds(pl.multiple_of(src * rk, rk), rk)
        return pltpu.make_async_remote_copy(
            dall.at[at], dall.at[at], d_send.at[d], d_recv.at[d], device_id=fs_peer(d), device_id_type=MESH
        )

    for d in range(1, NFS):
        d_copy(d, fs).start()
    for d in range(1, NFS):
        d_copy(d, fs_source(d)).wait_recv()

    rotated = dall[...]
    wide = rotated.astype(F32)
    cb[0] = jnp.sum((wide * wide).reshape(rank // 8, 8, width), axis=0)

    def c_copy(e):
        return pltpu.make_async_remote_copy(
            cb.at[0], cb.at[e], c_send.at[e], c_recv.at[e], device_id=tp_peer(e), device_id_type=MESH
        )

    for e in range(1, 2 * NZ):
        c_copy(e).start()

    for k in range(1, NX):
        for m in range(2):
            m_copy(m, fs_source(k), mf_send, mf_recv, k, fs_peer(k)).wait_recv()
        for j in range(1, NY):
            m_copy(0, fs_source(k), md_send, md_recv, j * NX + k, fs_peer(j * NX)).start()
    for k in range(1, NY):
        for m in range(2):
            m_copy(m, fs_source(k * NX), mf_send, mf_recv, k * NX, fs_peer(k * NX)).wait_recv()
        for j in range(1, NX):
            m_copy(1, fs_source(k * NX), md_send, md_recv, k * NX + j, fs_peer(j)).start()

    po_copy.wait_recv()
    turned = rotated.T
    for m in range(2):
        raws[m] = lax.dot_general(
            turned[m * half : (m + 1) * half], pboth[m], (((1,), (1,)), ((), ())), preferred_element_type=F32
        )

    squares = cb[0]
    for e in range(1, 2 * NZ):
        c_copy(e).wait_recv()
        squares = squares + cb[e]
    clip_level = CLIP_SHARE * math.sqrt(rank * width * NZ)
    factors = []
    for m in range(2):
        norm = jnp.sqrt(jnp.sum(squares[:, m * half : (m + 1) * half], axis=(0, 1), keepdims=True))
        factors.append(clip_level / jnp.maximum(norm, clip_level))
    steps = (sg_out, so_out)
    news = (gn_out, on_out)
    for m in range(2):
        step = raws[m, :, own_lanes] * factors[m]
        steps[m][...] = step
        news[m][...] = masters[m, :, own_lanes] - LEARN_RATE * step
    for d in range(1, NFS):
        if d // NX and d % NX:
            for m in range(2):
                m_copy(m, fs_source(d), md_send, md_recv, d, fs_peer(d)).wait_recv()
    for m in range(2):
        ebuf[m] = (masters[m] - LEARN_RATE * (raws[m] * factors[m])).astype(BF16)

    for d in axis_offsets:
        p_copy(fs, 0, rows, pf_send, pf_recv, d, fs_peer(d)).wait_send()
        for m in range(2):
            m_copy(m, fs, mf_send, mf_recv, d, fs_peer(d)).wait_send()
    po_copy.wait_send()
    for d in range(1, NFS):
        if d // NX and d % NX:
            p_copy(fs, 0, hr, pa_send, pa_recv, d, fs_peer(d)).wait_send()
            p_copy(fs, hr, hr, pb_send, pb_recv, d, fs_peer(d)).wait_send()
            for m in range(2):
                m_copy(m, fs, md_send, md_recv, d, fs_peer(d)).wait_send()
        rs_copy(d, fs).wait_send()
        d_copy(d, fs).wait_send()
    for e in range(1, 2 * NZ):
        z_copy(e).wait_send()
        c_copy(e).wait_send()
    for copy in swaps(x_hbm, g_hbm):
        copy.wait_send()


def store_kernel(*refs):
    count = (len(refs) - 2) // 2
    ins, outs, sem = refs[:count], refs[count:-1], refs[-1]
    sources = [*ins[:-1], ins[-1].at[0], ins[-1].at[1]]
    copies = [pltpu.make_async_copy(src, dst, sem.at[i]) for i, (src, dst) in enumerate(zip(sources, outs))]
    for copy in copies:
        copy.start()
    for copy in copies:
        copy.wait()


def shards(sizes, x, g, cv, b, proj, fm, sm, gm, om):
    NY, NX, NZ = sizes
    NFS = NY * NX
    tokens, d_model = x.shape
    channels = g.shape[1]
    rows, _, rank = proj.shape
    rk = rank // NFS
    cols = gm.shape[1]
    width = 2 * cols
    vmem = pl.BlockSpec(memory_space=pltpu.VMEM)
    hbm = pl.BlockSpec(memory_space=pltpu.HBM)
    dma = pltpu.SemaphoreType.DMA
    small = jax.ShapeDtypeStruct(fm.shape, F32)
    block = jax.ShapeDtypeStruct((cols, rows), F32)
    copy = jax.ShapeDtypeStruct((cols, d_model), BF16)
    results = pl.pallas_call(
        functools.partial(kernel, sizes),
        out_shape=(small, small, block, block, block, block, jax.ShapeDtypeStruct((2, cols, d_model), BF16)),
        in_specs=[hbm] * 9,
        out_specs=(vmem,) * 7,
        scratch_shapes=[
            pltpu.VMEM(proj.shape, BF16),
            pltpu.VMEM(fm.shape, F32),
            pltpu.VMEM(sm.shape, F32),
            pltpu.VMEM((2, tokens, d_model), BF16),
            pltpu.VMEM((2, tokens, channels), BF16),
            pltpu.VMEM((2, d_model, rank), BF16),
            pltpu.VMEM((2, cols, d_model), F32),
            pltpu.VMEM((2, cols, d_model), F32),
            pltpu.VMEM((2 * tokens, rank), F32),
            pltpu.VMEM((rank, channels), F32),
            pltpu.VMEM((rank, channels), BF16),
            pltpu.VMEM((NFS, rk, channels), BF16),
            pltpu.VMEM((rk, channels), F32),
            pltpu.VMEM((rk, channels), BF16),
            pltpu.VMEM((2 * NZ, rk, width), BF16),
            pltpu.VMEM((rank, width), BF16),
            pltpu.VMEM((2 * NZ, 8, width), F32),
            dma((7,)),
            dma((2,)),
            dma((2,)),
        ]
        + [dma((NFS,))] * 8
        + [dma((2 * NZ,))] * 2
        + [dma((NFS,))] * 2
        + [dma((2 * NZ,))] * 2
        + [dma((2,))]
        + [dma((2, NFS))] * 4
        + [pltpu.SemaphoreType.REGULAR((4,))],
        compiler_params=pltpu.CompilerParams(collective_id=0, has_side_effects=True, vmem_limit_bytes=48 * 2**20),
    )(*(pltpu.with_memory_space_constraint(a, pltpu.HBM) for a in (x, g, cv, b, proj, fm, sm, gm.T, om)))
    fn, sn, sg, so, gn, on, gc, oc = pl.pallas_call(
        store_kernel,
        out_shape=(small, small, block, block, block, block, copy, copy),
        in_specs=[vmem] * 7,
        out_specs=(hbm,) * 8,
        scratch_shapes=[dma((8,))],
        compiler_params=pltpu.CompilerParams(vmem_limit_bytes=2**20),
    )(*results)
    return fn, sn, sg.T, so, gn.T, on, gc.T, oc


def solution(mesh):
    sizes = (4, 4, 8)
    split = Mesh(mesh.devices.reshape(*sizes, 2), FS_TP)
    return build(split, sizes)


def build(split, sizes):
    in_specs = (
        P(FS_TP, None),
        P(FS_TP, None),
        P(FS_TP, None),
        P(FS_TP, None),
        P(FS, None, None),
        P(FS, None, TP),
        P(FS, None, TP),
        P(FS, TP),
        P(TP, FS),
    )
    out_specs = (
        P(FS, None, TP),
        P(FS, None, TP),
        P(FS, TP),
        P(TP, FS),
        P(FS, TP),
        P(TP, FS),
        P(None, TP),
        P(TP, None),
    )
    return jax.shard_map(
        functools.partial(shards, sizes), mesh=split, in_specs=in_specs, out_specs=out_specs, check_vma=False
    )
```

```python
import functools
import math

import jax
import jax.numpy as jnp
from jax import lax
from jax.experimental import pallas as pl
from jax.experimental.pallas import tpu as pltpu
from jax.sharding import Mesh
from jax.sharding import PartitionSpec as P

MESH = pl.DeviceIdType.MESH
F32 = jnp.float32
BF16 = jnp.bfloat16
FS = ("y", "x")
TP = ("z", "c")
FS_TP = ("y", "x", "z", "c")

BETA_FIRST = 0.8
BETA_SECOND = 0.9
LEARN_RATE = 0.01
CLIP_SHARE = 0.5


def kernel(
    sizes,
    x_hbm,
    g_hbm,
    cv_hbm,
    b_hbm,
    proj_hbm,
    fm_hbm,
    sm_hbm,
    gm_hbm,
    om_hbm,
    fn_out,
    sn_out,
    sg_out,
    so_out,
    gn_out,
    on_out,
    ebuf,
    proj,
    fm,
    sm,
    ax,
    ag,
    pboth,
    masters,
    raws,
    mix,
    low,
    lowb,
    rs,
    psf,
    psb,
    zb,
    dall,
    cb,
    load_sem,
    swap_send,
    swap_recv,
    p_send,
    pf_recv,
    pd_recv,
    rs_send,
    rs_recv,
    z_send,
    z_recv,
    d_send,
    d_recv,
    c_send,
    c_recv,
    po_sem,
    mf_send,
    mf_recv,
    md_send,
    md_recv,
    line_sem,
):
    NY, NX, NZ = sizes
    NFS = NY * NX
    tokens = x_hbm.shape[0]
    rows = proj.shape[0]
    rank = 2 * pboth.shape[3]
    rk = rank // NFS
    width = zb.shape[-1]
    half = width // 2
    y, x = lax.axis_index("y"), lax.axis_index("x")
    z, c = lax.axis_index("z"), lax.axis_index("c")
    fs = y * NX + x
    pfull = pboth.at[c]
    own = pl.multiple_of(fs * rows, rows)
    own_lanes = pl.ds(own, rows)

    def fs_peer(d):
        return (lax.rem(y + d // NX, NY), lax.rem(x + d % NX, NX), z, c)

    def fs_source(d):
        return lax.rem(y + NY - d // NX, NY) * NX + lax.rem(x + NX - d % NX, NX)

    def tp_peer(e):
        return (y, x, lax.rem(z + e // 2, NZ), lax.rem(c + e % 2, 2))

    partner = (y, x, z, 1 - c)

    def hops(k, n):
        return min(k, n - k)

    fs_offsets = sorted(range(1, NFS), key=lambda d: -hops(d // NX, NY) - hops(d % NX, NX))
    tp_offsets = sorted(range(1, 2 * NZ), key=lambda e: -2 * hops(e // 2, NZ) - e % 2)
    y_offsets = sorted(range(1, NY), key=lambda j: -hops(j, NY))
    x_offsets = sorted(range(1, NX), key=lambda j: -hops(j, NX))

    def own_loads(act, cot):
        return (
            pltpu.make_async_copy(act, ax.at[0], load_sem.at[0]),
            pltpu.make_async_copy(cot, ag.at[0], load_sem.at[1]),
        )

    def swaps(act, cot):
        return (
            pltpu.make_async_remote_copy(
                act, ax.at[1], swap_send.at[0], swap_recv.at[0], device_id=partner, device_id_type=MESH
            ),
            pltpu.make_async_remote_copy(
                cot, ag.at[1], swap_send.at[1], swap_recv.at[1], device_id=partner, device_id_type=MESH
            ),
        )

    proj_load = pltpu.make_async_copy(proj_hbm, proj, load_sem.at[2])
    proj_load.start()
    axis_offsets = [k for k in range(1, NX)] + [k * NX for k in range(1, NY)]
    z_neighbours = ((y, x, lax.rem(z + 1, NZ), c), (y, x, lax.rem(z + NZ - 1, NZ), c))
    greeted = [fs_peer(d) for d in axis_offsets] + [partner, *z_neighbours]
    barrier = pltpu.get_barrier_semaphore()
    for peer in greeted:
        pl.semaphore_signal(barrier, inc=1, device_id=peer, device_id_type=MESH)

    @pl.when(c == 0)
    def _():
        for copy in own_loads(x_hbm, g_hbm):
            copy.start()

    @pl.when(c == 1)
    def _():
        for copy in own_loads(b_hbm, cv_hbm):
            copy.start()

    late_loads = [
        pltpu.make_async_copy(src, dst, load_sem.at[3 + i])
        for i, (src, dst) in enumerate(
            ((fm_hbm, fm), (sm_hbm, sm), (gm_hbm, masters.at[0, :, own_lanes]), (om_hbm, masters.at[1, :, own_lanes]))
        )
    ]
    for copy in late_loads:
        copy.start()

    def line_signal(r):
        for peer in z_neighbours:
            pl.semaphore_signal(line_sem.at[r], inc=1, device_id=peer, device_id_type=MESH)

    def line_wait(r):
        pl.semaphore_wait(line_sem.at[r], 2)

    def arrived(like, sem):
        pltpu.make_async_copy(like, like, sem).wait()

    hk, half_rank = rk // 2, rank // 2
    natural = lax.broadcasted_iota(jnp.int32, (rank, rank), 0)
    place = lax.broadcasted_iota(jnp.int32, (rank, rank), 1)
    inner = lax.rem(place, half_rank)
    wanted = lax.div(inner, hk) * rk + lax.div(place, half_rank) * hk + lax.rem(inner, hk)
    order = jnp.where(natural == wanted, 1.0, 0.0).astype(BF16)
    proj_load.wait()
    slab = jnp.where(c == 0, proj[:, 0, :], proj[:, 1, :])
    slab = jnp.dot(slab, order, preferred_element_type=F32).astype(BF16)
    for h in range(2):
        pfull[h, own_lanes, :] = slab[:, h * half_rank : (h + 1) * half_rank]
    pl.semaphore_wait(barrier, len(greeted))
    line_signal(0)

    def p_copy(h, src, first, count, recv, peer):
        at = pl.ds(pl.multiple_of(src * rows + first, count), count)
        return pltpu.make_async_remote_copy(
            pfull.at[h, at], pfull.at[h, at], p_send.at[h], recv, device_id=peer, device_id_type=MESH
        )

    hr = rows // 2
    for h in range(2):
        for d in axis_offsets:
            p_copy(h, fs, 0, rows, pf_recv.at[h, d], fs_peer(d)).start()

    @pl.when(c == 0)
    def _():
        for copy in swaps(b_hbm, cv_hbm):
            copy.start()

    @pl.when(c == 1)
    def _():
        for copy in swaps(x_hbm, g_hbm):
            copy.start()

    for h in range(2):
        for k in range(1, max(NX, NY)):
            if k < NX:
                p_copy(h, fs_source(k), 0, rows, pf_recv.at[h, k], fs_peer(k)).wait_recv()
                for j in y_offsets:
                    p_copy(h, fs_source(k), 0, hr, pd_recv.at[h, j], fs_peer(j * NX)).start()
            if k < NY:
                p_copy(h, fs_source(k * NX), 0, rows, pf_recv.at[h, k * NX], fs_peer(k * NX)).wait_recv()
                for j in x_offsets:
                    p_copy(h, fs_source(k * NX), hr, hr, pd_recv.at[h, k], fs_peer(j)).start()

    line_wait(0)
    line_signal(1)
    for copy in own_loads(x_hbm, g_hbm):
        copy.wait()
    for copy in swaps(x_hbm, g_hbm):
        copy.wait_recv()

    def rs_copy(h, d, dst):
        return pltpu.make_async_remote_copy(
            lowb.at[h, dst], rs.at[h, d], rs_send.at[h], rs_recv.at[h], device_id=fs_peer(d), device_id_type=MESH
        )

    def fs_target(d):
        return lax.rem(y + d // NX, NY) * NX + lax.rem(x + d % NX, NX)

    turn = (((0,), (0,)), ((), ()))
    for h in range(2):
        for dy in range(NY):
            if dy > 0:
                arrived(pfull.at[h, pl.ds(0, (NX - 1) * rows)], pd_recv.at[h, dy])
            ydim = lax.rem(y + NY - dy, NY)
            at = pl.ds(pl.multiple_of(ydim * (NX * rows), NX * rows), NX * rows)
            for s in range(2):
                term = jnp.dot(ax[s, :, at], pfull[h, at, :], preferred_element_type=F32)
                span = pl.ds(s * tokens, tokens)
                if dy == 0:
                    mix[span, :] = term
                else:
                    mix[span, :] += term

        both = mix[...]
        upper = both.astype(BF16)
        lower = (both - upper.astype(F32)).astype(BF16)
        cots = ag[...].reshape(2 * tokens, ag.shape[-1])
        part = lax.dot_general(upper, cots, turn, preferred_element_type=F32) + lax.dot_general(
            lower, cots, turn, preferred_element_type=F32
        )
        low[h] = part.reshape(NFS, hk, part.shape[-1])
        lowb[h] = low[h].astype(BF16)
        for d in fs_offsets:
            rs_copy(h, d, fs_target(d)).start()
        line_wait(1 + h)
        line_signal(2 + h)

    po_copy = pltpu.make_async_remote_copy(
        pfull, pfull, po_sem.at[0], po_sem.at[1], device_id=partner, device_id_type=MESH
    )
    po_copy.start()

    sums = []
    for h in range(2):
        total = low[h, fs]
        arrived(rs.at[h, pl.ds(1, NFS - 1)], rs_recv.at[h])
        for d in range(1, NFS):
            total = total + rs[h, d].astype(F32)
        sums.append(total)
    top, bottom = sums
    left = lax.rem(lax.broadcasted_iota(jnp.int32, top.shape, 1), width) < half
    psf[0] = jnp.where(left, top, pltpu.roll(bottom, half, 1))
    psf[1] = jnp.where(left, pltpu.roll(top, top.shape[1] - half, 1), bottom)
    psb[...] = psf[...].astype(BF16)

    def z_copy(e):
        zt = lax.rem(z + e // 2, NZ)
        return pltpu.make_async_remote_copy(
            psb.at[lax.rem(c + e % 2, 2), :, pl.ds(pl.multiple_of(zt * width, width), width)],
            zb.at[e],
            z_send,
            z_recv,
            device_id=tp_peer(e),
            device_id_type=MESH,
        )

    line_wait(3)
    for e in tp_offsets:
        z_copy(e).start()

    for copy in late_loads:
        copy.wait()

    def m_copy(m, src, send, recv, peer):
        at = pl.ds(pl.multiple_of(src * rows, rows), rows)
        return pltpu.make_async_remote_copy(
            masters.at[m, :, at], masters.at[m, :, at], send, recv, device_id=peer, device_id_type=MESH
        )

    for d in axis_offsets:
        for m in range(2):
            m_copy(m, fs, mf_send, mf_recv, fs_peer(d)).start()

    same = psf[c, :, pl.ds(pl.multiple_of(z * width, width), width)]
    other = jnp.zeros_like(same)
    arrived(zb.at[pl.ds(1, 2 * NZ - 1)], z_recv)
    for e in range(1, 2 * NZ):
        if e % 2:
            other = other + zb[e].astype(F32)
        else:
            same = same + zb[e].astype(F32)

    fm_in, sm_in = fm[...], sm[...]
    directions = []
    for m in range(2):
        packed = jnp.where(c == m, same, other)
        part = jnp.concatenate([packed[:, :half], packed[:, half:]], axis=0)
        first = BETA_FIRST * fm_in[:, m, :] + (1.0 - BETA_FIRST) * part
        second = BETA_SECOND * sm_in[:, m, :] + (1.0 - BETA_SECOND) * part * part
        fn_out[:, m, :] = first
        sn_out[:, m, :] = second
        directions.append(first / jnp.sqrt(second))
    mine = pl.ds(pl.multiple_of(fs * rk, rk), rk)
    dall[mine, :] = jnp.concatenate(directions, axis=1).astype(BF16)

    def d_copy(d):
        at = pl.ds(pl.multiple_of(fs * rk, rk), rk)
        return pltpu.make_async_remote_copy(
            dall.at[at], dall.at[at], d_send, d_recv, device_id=fs_peer(d), device_id_type=MESH
        )

    for d in fs_offsets:
        d_copy(d).start()

    arrived(masters.at[:, :, pl.ds(0, len(axis_offsets) * rows)], mf_recv)
    for k in range(1, NX):
        for j in y_offsets:
            m_copy(0, fs_source(k), md_send, md_recv, fs_peer(j * NX)).start()
    for k in range(1, NY):
        for j in x_offsets:
            m_copy(1, fs_source(k * NX), md_send, md_recv, fs_peer(j)).start()

    arrived(dall.at[pl.ds(0, (NFS - 1) * rk)], d_recv)

    rotated = dall[...]
    wide = rotated.astype(F32)
    cb[0] = jnp.sum(wide * wide, axis=0, keepdims=True)

    def c_copy(e):
        return pltpu.make_async_remote_copy(
            cb.at[0], cb.at[e], c_send, c_recv, device_id=tp_peer(e), device_id_type=MESH
        )

    for e in tp_offsets:
        c_copy(e).start()

    po_copy.wait_recv()
    turned = lax.dot_general(rotated, order, turn, preferred_element_type=F32).astype(BF16)
    for m in range(2):
        lhs = turned[m * half : (m + 1) * half]
        across = (((1,), (1,)), ((), ()))
        raws[m] = lax.dot_general(
            lhs[:, :half_rank], pboth[m, 0], across, preferred_element_type=F32
        ) + lax.dot_general(lhs[:, half_rank:], pboth[m, 1], across, preferred_element_type=F32)

    squares = cb[0]
    arrived(cb.at[pl.ds(1, 2 * NZ - 1)], c_recv)
    for e in range(1, 2 * NZ):
        squares = squares + cb[e]
    clip_level = CLIP_SHARE * math.sqrt(rank * width * NZ)
    factors = []
    for m in range(2):
        norm = jnp.sqrt(jnp.sum(squares[:, m * half : (m + 1) * half], axis=(0, 1), keepdims=True))
        factors.append(clip_level / jnp.maximum(norm, clip_level))
    steps = (sg_out, so_out)
    news = (gn_out, on_out)
    for m in range(2):
        step = raws[m, :, own_lanes] * factors[m]
        steps[m][...] = step
        news[m][...] = masters[m, :, own_lanes] - LEARN_RATE * step
    diagonal = (NY - 1) * (NX - 1)
    arrived(masters.at[:, :, pl.ds(0, diagonal * rows)], md_recv)
    for m in range(2):
        ebuf[m] = (masters[m] - LEARN_RATE * (raws[m] * factors[m])).astype(BF16)

    for h in range(2):
        arrived(pfull.at[h, pl.ds(0, (NFS - 1) * rows)], p_send.at[h])
        arrived(rs.at[h, pl.ds(1, NFS - 1)], rs_send.at[h])
    po_copy.wait_send()
    arrived(zb.at[pl.ds(1, 2 * NZ - 1)], z_send)
    arrived(masters.at[:, :, pl.ds(0, len(axis_offsets) * rows)], mf_send)
    arrived(dall.at[pl.ds(0, (NFS - 1) * rk)], d_send)
    arrived(masters.at[:, :, pl.ds(0, diagonal * rows)], md_send)
    arrived(cb.at[pl.ds(1, 2 * NZ - 1)], c_send)
    for copy in swaps(x_hbm, g_hbm):
        copy.wait_send()


def store_kernel(*refs):
    count = (len(refs) - 2) // 2
    ins, outs, sem = refs[:count], refs[count:-1], refs[-1]
    sources = [*ins[:-1], ins[-1].at[0], ins[-1].at[1]]
    copies = [pltpu.make_async_copy(src, dst, sem.at[i]) for i, (src, dst) in enumerate(zip(sources, outs))]
    for copy in copies:
        copy.start()
    for copy in copies:
        copy.wait()


def shards(sizes, x, g, cv, b, proj, fm, sm, gm, om):
    NY, NX, NZ = sizes
    NFS = NY * NX
    tokens, d_model = x.shape
    channels = g.shape[1]
    rows, _, rank = proj.shape
    rk = rank // NFS
    cols = gm.shape[1]
    width = 2 * cols
    vmem = pl.BlockSpec(memory_space=pltpu.VMEM)
    hbm = pl.BlockSpec(memory_space=pltpu.HBM)
    dma = pltpu.SemaphoreType.DMA
    small = jax.ShapeDtypeStruct(fm.shape, F32)
    block = jax.ShapeDtypeStruct((cols, rows), F32)
    copy = jax.ShapeDtypeStruct((cols, d_model), BF16)
    results = pl.pallas_call(
        functools.partial(kernel, sizes),
        out_shape=(small, small, block, block, block, block, jax.ShapeDtypeStruct((2, cols, d_model), BF16)),
        in_specs=[hbm] * 9,
        out_specs=(vmem,) * 7,
        scratch_shapes=[
            pltpu.VMEM(proj.shape, BF16),
            pltpu.VMEM(fm.shape, F32),
            pltpu.VMEM(sm.shape, F32),
            pltpu.VMEM((2, tokens, d_model), BF16),
            pltpu.VMEM((2, tokens, channels), BF16),
            pltpu.VMEM((2, 2, d_model, rank // 2), BF16),
            pltpu.VMEM((2, cols, d_model), F32),
            pltpu.VMEM((2, cols, d_model), F32),
            pltpu.VMEM((2 * tokens, rank // 2), F32),
            pltpu.VMEM((2, NFS, rk // 2, channels), F32),
            pltpu.VMEM((2, NFS, rk // 2, channels), BF16),
            pltpu.VMEM((2, NFS, rk // 2, channels), BF16),
            pltpu.VMEM((2, rk // 2, channels), F32),
            pltpu.VMEM((2, rk // 2, channels), BF16),
            pltpu.VMEM((2 * NZ, rk // 2, width), BF16),
            pltpu.VMEM((rank, width), BF16),
            pltpu.VMEM((2 * NZ, 1, width), F32),
            dma((7,)),
            dma((2,)),
            dma((2,)),
        ]
        + [dma((2,)), dma((2, NFS)), dma((2, NY))]
        + [dma((2,))] * 2
        + [dma] * 6
        + [dma((2,))]
        + [dma] * 4
        + [pltpu.SemaphoreType.REGULAR((4,))],
        compiler_params=pltpu.CompilerParams(collective_id=0, has_side_effects=True, vmem_limit_bytes=48 * 2**20),
    )(*(pltpu.with_memory_space_constraint(a, pltpu.HBM) for a in (x, g, cv, b, proj, fm, sm, gm.T, om)))
    fn, sn, sg, so, gn, on, gc, oc = pl.pallas_call(
        store_kernel,
        out_shape=(small, small, block, block, block, block, copy, copy),
        in_specs=[vmem] * 7,
        out_specs=(hbm,) * 8,
        scratch_shapes=[dma((8,))],
        compiler_params=pltpu.CompilerParams(vmem_limit_bytes=2**20),
    )(*results)
    return fn, sn, sg.T, so, gn.T, on, gc.T, oc


def solution(mesh):
    sizes = (4, 4, 8)
    split = Mesh(mesh.devices.reshape(*sizes, 2), FS_TP)
    return build(split, sizes)


def build(split, sizes):
    in_specs = (
        P(FS_TP, None),
        P(FS_TP, None),
        P(FS_TP, None),
        P(FS_TP, None),
        P(FS, None, None),
        P(FS, None, TP),
        P(FS, None, TP),
        P(FS, TP),
        P(TP, FS),
    )
    out_specs = (
        P(FS, None, TP),
        P(FS, None, TP),
        P(FS, TP),
        P(TP, FS),
        P(FS, TP),
        P(TP, FS),
        P(None, TP),
        P(TP, None),
    )
    return jax.shard_map(
        functools.partial(shards, sizes), mesh=split, in_specs=in_specs, out_specs=out_specs, check_vma=False
    )
```

```python
import functools
import math

import jax
import jax.numpy as jnp
from jax import lax
from jax.experimental import pallas as pl
from jax.experimental.pallas import tpu as pltpu
from jax.sharding import Mesh
from jax.sharding import PartitionSpec as P

MESH = pl.DeviceIdType.MESH
F32 = jnp.float32
BF16 = jnp.bfloat16
FS = ("y", "x")
TP = ("z", "c")
FS_TP = ("y", "x", "z", "c")

BETA_FIRST = 0.8
BETA_SECOND = 0.9
LEARN_RATE = 0.01
CLIP_SHARE = 0.5


def kernel(
    sizes,
    x_hbm,
    g_hbm,
    cv_hbm,
    b_hbm,
    proj_hbm,
    fm_hbm,
    sm_hbm,
    gm_hbm,
    om_hbm,
    fn_out,
    sn_out,
    sg_out,
    so_out,
    gn_out,
    on_out,
    ebuf,
    proj,
    fm,
    sm,
    ax,
    ag,
    pboth,
    masters,
    raws,
    mix,
    low,
    lowb,
    rs,
    psf,
    psb,
    zb,
    dall,
    cb,
    load_sem,
    swap_send,
    swap_recv,
    p_send,
    pf_recv,
    pd_recv,
    rs_send,
    rs_recv,
    z_send,
    z_recv,
    d_send,
    d_recv,
    c_send,
    c_recv,
    po_sem,
    mf_send,
    mf_recv,
    md_send,
    md_recv,
    line_sem,
):
    NY, NX, NZ = sizes
    NFS = NY * NX
    tokens = x_hbm.shape[0]
    rows = proj.shape[0]
    rank = 2 * pboth.shape[2]
    rk = rank // NFS
    width = zb.shape[-1]
    half = width // 2
    y, x = lax.axis_index("y"), lax.axis_index("x")
    z, c = lax.axis_index("z"), lax.axis_index("c")
    fs = y * NX + x
    pfull = pboth.at[c]
    own = pl.multiple_of(fs * rows, rows)
    own_lanes = pl.ds(own, rows)

    def fs_peer(d):
        return (lax.rem(y + d // NX, NY), lax.rem(x + d % NX, NX), z, c)

    def fs_source(d):
        return lax.rem(y + NY - d // NX, NY) * NX + lax.rem(x + NX - d % NX, NX)

    def tp_peer(e):
        return (y, x, lax.rem(z + e // 2, NZ), lax.rem(c + e % 2, 2))

    partner = (y, x, z, 1 - c)

    def hops(k, n):
        return min(k, n - k)

    fs_offsets = sorted(range(1, NFS), key=lambda d: -hops(d // NX, NY) - hops(d % NX, NX))
    tp_offsets = sorted(range(1, 2 * NZ), key=lambda e: -2 * hops(e // 2, NZ) - e % 2)
    y_offsets = sorted(range(1, NY), key=lambda j: -hops(j, NY))
    x_offsets = sorted(range(1, NX), key=lambda j: -hops(j, NX))

    def own_loads(act, cot):
        return (
            pltpu.make_async_copy(act, ax.at[0], load_sem.at[0]),
            pltpu.make_async_copy(cot, ag.at[0], load_sem.at[1]),
        )

    def swaps(act, cot):
        return (
            pltpu.make_async_remote_copy(
                act, ax.at[1], swap_send.at[0], swap_recv.at[0], device_id=partner, device_id_type=MESH
            ),
            pltpu.make_async_remote_copy(
                cot, ag.at[1], swap_send.at[1], swap_recv.at[1], device_id=partner, device_id_type=MESH
            ),
        )

    proj_load = pltpu.make_async_copy(proj_hbm, proj, load_sem.at[2])
    proj_load.start()
    axis_offsets = [k for k in range(1, NX)] + [k * NX for k in range(1, NY)]
    near = [k for k in range(1, NZ) if hops(k, NZ) <= 2]
    relays = [(y, x, lax.rem(z + k, NZ), c) for k in near if hops(k, NZ) == 2]
    greeted = [fs_peer(d) for d in axis_offsets] + [partner] + [tp_peer(2 * k + i) for k in near for i in range(2)]
    barrier = pltpu.get_barrier_semaphore()
    for peer in greeted:
        pl.semaphore_signal(barrier, inc=1, device_id=peer, device_id_type=MESH)

    @pl.when(c == 0)
    def _():
        for copy in own_loads(x_hbm, g_hbm):
            copy.start()

    @pl.when(c == 1)
    def _():
        for copy in own_loads(b_hbm, cv_hbm):
            copy.start()

    late_loads = [
        pltpu.make_async_copy(src, dst, load_sem.at[3 + i])
        for i, (src, dst) in enumerate(
            ((fm_hbm, fm), (sm_hbm, sm), (gm_hbm, masters.at[0, :, own_lanes]), (om_hbm, masters.at[1, :, own_lanes]))
        )
    ]
    for copy in late_loads:
        copy.start()

    def arrived(like, sem):
        pltpu.make_async_copy(like, like, sem).wait()

    hk, half_rank = rk // 2, rank // 2
    natural = lax.broadcasted_iota(jnp.int32, (rank, rank), 0)
    place = lax.broadcasted_iota(jnp.int32, (rank, rank), 1)
    inner = lax.rem(place, half_rank)
    wanted = lax.div(inner, hk) * rk + lax.div(place, half_rank) * hk + lax.rem(inner, hk)
    order = jnp.where(natural == wanted, 1.0, 0.0).astype(BF16)
    proj_load.wait()
    slab = jnp.where(c == 0, proj[:, 0, :], proj[:, 1, :])
    slab = lax.dot_general(order, slab, (((0,), (1,)), ((), ())), preferred_element_type=F32).astype(BF16)
    for h in range(2):
        pfull[h, :, own_lanes] = slab[h * half_rank : (h + 1) * half_rank]
    pl.semaphore_wait(barrier, len(greeted))
    for peer in relays:
        pl.semaphore_signal(line_sem, inc=1, device_id=peer, device_id_type=MESH)

    def p_copy(h, src, first, count, recv, peer):
        at = pl.ds(pl.multiple_of(src * rows, rows), rows)
        ref = pfull.at[h, pl.ds(first, count), at]
        return pltpu.make_async_remote_copy(ref, ref, p_send.at[h], recv, device_id=peer, device_id_type=MESH)

    hr = half_rank // 2

    def p_first(h):
        for d in axis_offsets:
            p_copy(h, fs, 0, half_rank, pf_recv.at[h, axis_offsets.index(d)], fs_peer(d)).start()

    def p_onward(h, k):
        if k < NX:
            p_copy(h, fs_source(k), 0, half_rank, pf_recv.at[h, axis_offsets.index(k)], fs_peer(k)).wait_recv()
            for j in y_offsets:
                p_copy(h, fs_source(k), 0, hr, pd_recv.at[h, j], fs_peer(j * NX)).start()
        if k < NY:
            sem = pf_recv.at[h, axis_offsets.index(k * NX)]
            p_copy(h, fs_source(k * NX), 0, half_rank, sem, fs_peer(k * NX)).wait_recv()
            for j in x_offsets:
                p_copy(h, fs_source(k * NX), hr, hr, pd_recv.at[h, k], fs_peer(j)).start()

    p_first(0)

    @pl.when(c == 0)
    def _():
        for copy in swaps(b_hbm, cv_hbm):
            copy.start()

    @pl.when(c == 1)
    def _():
        for copy in swaps(x_hbm, g_hbm):
            copy.start()

    steps = sorted(range(1, max(NX, NY)), key=lambda k: hops(k, max(NX, NY)))
    p_first(1)
    for h in range(2):
        for k in steps:
            p_onward(h, k)

    for copy in own_loads(x_hbm, g_hbm):
        copy.wait()
    for copy in swaps(x_hbm, g_hbm):
        copy.wait_recv()

    def rs_copy(h, d, dst):
        return pltpu.make_async_remote_copy(
            lowb.at[h, dst], rs.at[h, d], rs_send.at[h], rs_recv.at[h], device_id=fs_peer(d), device_id_type=MESH
        )

    def fs_target(d):
        return lax.rem(y + d // NX, NY) * NX + lax.rem(x + d % NX, NX)

    across = (((1,), (1,)), ((), ()))

    def mix_slabs(h, dy):
        if dy > 0:
            arrived(pfull.at[h, :, pl.ds(0, (NX - 1) * rows)], pd_recv.at[h, dy])
        ydim = lax.rem(y + NY - dy, NY)
        at = pl.ds(pl.multiple_of(ydim * (NX * rows), NX * rows), NX * rows)
        for s in range(2):
            term = lax.dot_general(pfull[h, :, at], ax[s, :, at], across, preferred_element_type=F32)
            span = slice(s * tokens, (s + 1) * tokens)
            if dy == 0:
                mix[h, :, span] = term
            else:
                mix[h, :, span] += term

    for h in range(2):
        mix_slabs(h, 0)
    cots = ag[...].reshape(2 * tokens, ag.shape[-1])
    for h in range(2):
        for dy in range(1, NY):
            mix_slabs(h, dy)

        both = mix[h]
        upper = both.astype(BF16)
        lower = (both - upper.astype(F32)).astype(BF16)
        pair = jnp.dot(jnp.concatenate([upper, lower], axis=0), cots, preferred_element_type=F32)
        part = pair[:half_rank] + pair[half_rank:]
        low[h] = part.reshape(NFS, hk, part.shape[-1])
        lowb[h] = low[h].astype(BF16)
        for d in fs_offsets:
            rs_copy(h, d, fs_target(d)).start()

    po_copy = pltpu.make_async_remote_copy(
        pfull, pfull, po_sem.at[0], po_sem.at[1], device_id=partner, device_id_type=MESH
    )
    po_copy.start()

    sums = []
    for h in range(2):
        total = low[h, fs]
        arrived(rs.at[h, pl.ds(1, NFS - 1)], rs_recv.at[h])
        for d in range(1, NFS):
            total = total + rs[h, d].astype(F32)
        sums.append(total)
    top, bottom = sums
    left = lax.rem(lax.broadcasted_iota(jnp.int32, top.shape, 1), width) < half
    psf[0] = jnp.where(left, top, pltpu.roll(bottom, half, 1))
    psf[1] = jnp.where(left, pltpu.roll(top, top.shape[1] - half, 1), bottom)
    psb[...] = psf[...].astype(BF16)

    def z_copy(e):
        zt = lax.rem(z + e // 2, NZ)
        return pltpu.make_async_remote_copy(
            psb.at[lax.rem(c + e % 2, 2), :, pl.ds(pl.multiple_of(zt * width, width), width)],
            zb.at[e],
            z_send,
            z_recv,
            device_id=tp_peer(e),
            device_id_type=MESH,
        )

    pl.semaphore_wait(line_sem, len(relays))
    for e in tp_offsets:
        z_copy(e).start()

    for copy in late_loads:
        copy.wait()

    def m_copy(m, src, send, recv, peer):
        at = pl.ds(pl.multiple_of(src * rows, rows), rows)
        return pltpu.make_async_remote_copy(
            masters.at[m, :, at], masters.at[m, :, at], send, recv, device_id=peer, device_id_type=MESH
        )

    for d in axis_offsets:
        for m in range(2):
            m_copy(m, fs, mf_send, mf_recv, fs_peer(d)).start()

    same = psf[c, :, pl.ds(pl.multiple_of(z * width, width), width)]
    other = jnp.zeros_like(same)
    arrived(zb.at[pl.ds(1, 2 * NZ - 1)], z_recv)
    for e in range(1, 2 * NZ):
        if e % 2:
            other = other + zb[e].astype(F32)
        else:
            same = same + zb[e].astype(F32)

    fm_in, sm_in = fm[...], sm[...]
    directions = []
    for m in range(2):
        packed = jnp.where(c == m, same, other)
        part = jnp.concatenate([packed[:, :half], packed[:, half:]], axis=0)
        first = BETA_FIRST * fm_in[:, m, :] + (1.0 - BETA_FIRST) * part
        second = BETA_SECOND * sm_in[:, m, :] + (1.0 - BETA_SECOND) * part * part
        fn_out[:, m, :] = first
        sn_out[:, m, :] = second
        directions.append(first / jnp.sqrt(second))
    mine = pl.ds(pl.multiple_of(fs * rk, rk), rk)
    dall[mine, :] = jnp.concatenate(directions, axis=1).astype(BF16)

    def d_copy(d):
        at = pl.ds(pl.multiple_of(fs * rk, rk), rk)
        return pltpu.make_async_remote_copy(
            dall.at[at], dall.at[at], d_send, d_recv, device_id=fs_peer(d), device_id_type=MESH
        )

    for d in fs_offsets:
        d_copy(d).start()

    arrived(masters.at[:, :, pl.ds(0, len(axis_offsets) * rows)], mf_recv)
    for k in range(1, NX):
        for j in y_offsets:
            m_copy(0, fs_source(k), md_send, md_recv, fs_peer(j * NX)).start()
    for k in range(1, NY):
        for j in x_offsets:
            m_copy(1, fs_source(k * NX), md_send, md_recv, fs_peer(j)).start()

    arrived(dall.at[pl.ds(0, (NFS - 1) * rk)], d_recv)

    rotated = dall[...]
    wide = rotated.astype(F32)
    cb[0] = jnp.sum(wide * wide, axis=0, keepdims=True)

    def c_copy(e):
        return pltpu.make_async_remote_copy(
            cb.at[0], cb.at[e], c_send, c_recv, device_id=tp_peer(e), device_id_type=MESH
        )

    for e in tp_offsets:
        c_copy(e).start()

    po_copy.wait_recv()
    turned = lax.dot_general(rotated, order, (((0,), (0,)), ((), ())), preferred_element_type=F32).astype(BF16)
    for m in range(2):
        raws[m] = jnp.dot(
            turned[m * half : (m + 1) * half],
            pboth[m].reshape(rank, pboth.shape[-1]),
            preferred_element_type=F32,
        )

    squares = cb[0]
    arrived(cb.at[pl.ds(1, 2 * NZ - 1)], c_recv)
    for e in range(1, 2 * NZ):
        squares = squares + cb[e]
    clip_level = CLIP_SHARE * math.sqrt(rank * width * NZ)
    factors = []
    for m in range(2):
        norm = jnp.sqrt(jnp.sum(squares[:, m * half : (m + 1) * half], axis=(0, 1), keepdims=True))
        factors.append(clip_level / jnp.maximum(norm, clip_level))
    steps = (sg_out, so_out)
    news = (gn_out, on_out)
    for m in range(2):
        step = raws[m, :, own_lanes] * factors[m]
        steps[m][...] = step
        news[m][...] = masters[m, :, own_lanes] - LEARN_RATE * step
    diagonal = (NY - 1) * (NX - 1)
    arrived(masters.at[:, :, pl.ds(0, diagonal * rows)], md_recv)
    for m in range(2):
        ebuf[m] = (masters[m] - LEARN_RATE * (raws[m] * factors[m])).astype(BF16)

    for h in range(2):
        arrived(pfull.at[h, :, pl.ds(0, (NFS - 1) * rows)], p_send.at[h])
        arrived(rs.at[h, pl.ds(1, NFS - 1)], rs_send.at[h])
    po_copy.wait_send()
    arrived(zb.at[pl.ds(1, 2 * NZ - 1)], z_send)
    arrived(masters.at[:, :, pl.ds(0, len(axis_offsets) * rows)], mf_send)
    arrived(dall.at[pl.ds(0, (NFS - 1) * rk)], d_send)
    arrived(masters.at[:, :, pl.ds(0, diagonal * rows)], md_send)
    arrived(cb.at[pl.ds(1, 2 * NZ - 1)], c_send)
    for copy in swaps(x_hbm, g_hbm):
        copy.wait_send()


def store_kernel(*refs):
    count = (len(refs) - 2) // 2
    ins, outs, sem = refs[:count], refs[count:-1], refs[-1]
    sources = [*ins[:-1], ins[-1].at[0], ins[-1].at[1]]
    copies = [pltpu.make_async_copy(src, dst, sem.at[i]) for i, (src, dst) in enumerate(zip(sources, outs))]
    for copy in copies:
        copy.start()
    for copy in copies:
        copy.wait()


def shards(sizes, x, g, cv, b, proj, fm, sm, gm, om):
    NY, NX, NZ = sizes
    NFS = NY * NX
    tokens, d_model = x.shape
    channels = g.shape[1]
    rows, _, rank = proj.shape
    rk = rank // NFS
    cols = gm.shape[1]
    width = 2 * cols
    vmem = pl.BlockSpec(memory_space=pltpu.VMEM)
    hbm = pl.BlockSpec(memory_space=pltpu.HBM)
    dma = pltpu.SemaphoreType.DMA
    small = jax.ShapeDtypeStruct(fm.shape, F32)
    block = jax.ShapeDtypeStruct((cols, rows), F32)
    copy = jax.ShapeDtypeStruct((cols, d_model), BF16)
    results = pl.pallas_call(
        functools.partial(kernel, sizes),
        out_shape=(small, small, block, block, block, block, jax.ShapeDtypeStruct((2, cols, d_model), BF16)),
        in_specs=[hbm] * 9,
        out_specs=(vmem,) * 7,
        scratch_shapes=[
            pltpu.VMEM(proj.shape, BF16),
            pltpu.VMEM(fm.shape, F32),
            pltpu.VMEM(sm.shape, F32),
            pltpu.VMEM((2, tokens, d_model), BF16),
            pltpu.VMEM((2, tokens, channels), BF16),
            pltpu.VMEM((2, 2, rank // 2, d_model), BF16),
            pltpu.VMEM((2, cols, d_model), F32),
            pltpu.VMEM((2, cols, d_model), F32),
            pltpu.VMEM((2, rank // 2, 2 * tokens), F32),
            pltpu.VMEM((2, NFS, rk // 2, channels), F32),
            pltpu.VMEM((2, NFS, rk // 2, channels), BF16),
            pltpu.VMEM((2, NFS, rk // 2, channels), BF16),
            pltpu.VMEM((2, rk // 2, channels), F32),
            pltpu.VMEM((2, rk // 2, channels), BF16),
            pltpu.VMEM((2 * NZ, rk // 2, width), BF16),
            pltpu.VMEM((rank, width), BF16),
            pltpu.VMEM((2 * NZ, 1, width), F32),
            dma((7,)),
            dma((2,)),
            dma((2,)),
        ]
        + [dma((2,)), dma((2, NX + NY - 2)), dma((2, NY))]
        + [dma((2,))] * 2
        + [dma] * 6
        + [dma((2,))]
        + [dma] * 4
        + [pltpu.SemaphoreType.REGULAR],
        compiler_params=pltpu.CompilerParams(collective_id=0, has_side_effects=True, vmem_limit_bytes=48 * 2**20),
    )(*(pltpu.with_memory_space_constraint(a, pltpu.HBM) for a in (x, g, cv, b, proj, fm, sm, gm.T, om)))
    fn, sn, sg, so, gn, on, gc, oc = pl.pallas_call(
        store_kernel,
        out_shape=(small, small, block, block, block, block, copy, copy),
        in_specs=[vmem] * 7,
        out_specs=(hbm,) * 8,
        scratch_shapes=[dma((8,))],
        compiler_params=pltpu.CompilerParams(vmem_limit_bytes=2**20),
    )(*results)
    return fn, sn, sg.T, so, gn.T, on, gc.T, oc


def solution(mesh):
    sizes = (4, 4, 8)
    split = Mesh(mesh.devices.reshape(*sizes, 2), FS_TP)
    return build(split, sizes)


def build(split, sizes):
    in_specs = (
        P(FS_TP, None),
        P(FS_TP, None),
        P(FS_TP, None),
        P(FS_TP, None),
        P(FS, None, None),
        P(FS, None, TP),
        P(FS, None, TP),
        P(FS, TP),
        P(TP, FS),
    )
    out_specs = (
        P(FS, None, TP),
        P(FS, None, TP),
        P(FS, TP),
        P(TP, FS),
        P(FS, TP),
        P(TP, FS),
        P(None, TP),
        P(TP, None),
    )
    return jax.shard_map(
        functools.partial(shards, sizes), mesh=split, in_specs=in_specs, out_specs=out_specs, check_vma=False
    )
```

```python
import functools
import math

import jax
import jax.numpy as jnp
from jax import lax
from jax.experimental import pallas as pl
from jax.experimental.pallas import tpu as pltpu
from jax.sharding import Mesh
from jax.sharding import PartitionSpec as P

MESH = pl.DeviceIdType.MESH
F32 = jnp.float32
BF16 = jnp.bfloat16
FS = ("y", "x")
TP = ("z", "c")
FS_TP = ("y", "x", "z", "c")

BETA_FIRST = 0.8
BETA_SECOND = 0.9
LEARN_RATE = 0.01
CLIP_SHARE = 0.5


def kernel(
    sizes,
    x_hbm,
    g_hbm,
    cv_hbm,
    b_hbm,
    proj_hbm,
    fm_hbm,
    sm_hbm,
    gm_hbm,
    om_hbm,
    fn_out,
    sn_out,
    sg_out,
    so_out,
    gn_out,
    on_out,
    ebuf,
    proj,
    fm,
    sm,
    ax,
    ag,
    pboth,
    masters,
    raws,
    mix,
    low,
    lowb,
    rs,
    psf,
    psb,
    zb,
    dall,
    cb,
    fx,
    load_sem,
    swap_send,
    swap_recv,
    p_send,
    pf_recv,
    pd_recv,
    rs_send,
    rs_recv,
    z_send,
    z_recv,
    d_send,
    d_recv,
    c_send,
    c_recv,
    po_sem,
    mf_send,
    mf_recv,
    md_send,
    md_recv,
    line_sem,
    moment_send,
    moment_recv,
    back_sem,
):
    NY, NX, NZ = sizes
    NFS = NY * NX
    tokens = x_hbm.shape[0]
    rows = proj.shape[0]
    rank = 2 * pboth.shape[2]
    rk = rank // NFS
    width = zb.shape[-1]
    half = width // 2
    y, x = lax.axis_index("y"), lax.axis_index("x")
    z, c = lax.axis_index("z"), lax.axis_index("c")
    fs = y * NX + x
    pfull = pboth.at[c]
    own = pl.multiple_of(fs * rows, rows)
    own_lanes = pl.ds(own, rows)

    def fs_peer(d):
        return (lax.rem(y + d // NX, NY), lax.rem(x + d % NX, NX), z, c)

    def fs_source(d):
        return lax.rem(y + NY - d // NX, NY) * NX + lax.rem(x + NX - d % NX, NX)

    def tp_peer(e):
        return (y, x, lax.rem(z + e // 2, NZ), lax.rem(c + e % 2, 2))

    partner = (y, x, z, 1 - c)

    def hops(k, n):
        return min(k, n - k)

    fs_offsets = sorted(range(1, NFS), key=lambda d: -hops(d // NX, NY) - hops(d % NX, NX))
    z_offsets = sorted(range(1, NZ), key=lambda k: -hops(k, NZ))
    y_offsets = sorted(range(1, NY), key=lambda j: -hops(j, NY))
    x_offsets = sorted(range(1, NX), key=lambda j: -hops(j, NX))

    def own_loads(act, cot):
        return (
            pltpu.make_async_copy(act, ax.at[0], load_sem.at[0]),
            pltpu.make_async_copy(cot, ag.at[0], load_sem.at[1]),
        )

    def swaps(act, cot):
        return (
            pltpu.make_async_remote_copy(
                act, ax.at[1], swap_send.at[0], swap_recv.at[0], device_id=partner, device_id_type=MESH
            ),
            pltpu.make_async_remote_copy(
                cot, ag.at[1], swap_send.at[1], swap_recv.at[1], device_id=partner, device_id_type=MESH
            ),
        )

    proj_load = pltpu.make_async_copy(proj_hbm, proj, load_sem.at[2])
    proj_load.start()
    axis_offsets = [k for k in range(1, NX)] + [k * NX for k in range(1, NY)]
    near = [k for k in range(1, NZ) if hops(k, NZ) <= 2]
    relays = [(y, x, lax.rem(z + k, NZ), c) for k in near if hops(k, NZ) == 2]
    greeted = [fs_peer(d) for d in axis_offsets] + [partner] + [tp_peer(2 * k + i) for k in near for i in range(2)]
    barrier = pltpu.get_barrier_semaphore()
    for peer in greeted:
        pl.semaphore_signal(barrier, inc=1, device_id=peer, device_id_type=MESH)

    @pl.when(c == 0)
    def _():
        for copy in own_loads(x_hbm, g_hbm):
            copy.start()

    @pl.when(c == 1)
    def _():
        for copy in own_loads(b_hbm, cv_hbm):
            copy.start()

    late_loads = [
        pltpu.make_async_copy(src, dst, load_sem.at[3 + i])
        for i, (src, dst) in enumerate(
            ((fm_hbm, fm.at[c]), (sm_hbm, sm.at[c]), (gm_hbm, masters.at[0, :, own_lanes]), (om_hbm, masters.at[1, :, own_lanes]))
        )
    ]
    for copy in late_loads:
        copy.start()

    def arrived(like, sem):
        pltpu.make_async_copy(like, like, sem).wait()

    hk, half_rank = rk // 2, rank // 2
    natural = lax.broadcasted_iota(jnp.int32, (rank, rank), 0)
    place = lax.broadcasted_iota(jnp.int32, (rank, rank), 1)
    inner = lax.rem(place, half_rank)
    wanted = lax.div(inner, hk) * rk + lax.div(place, half_rank) * hk + lax.rem(inner, hk)
    order = jnp.where(natural == wanted, 1.0, 0.0).astype(BF16)
    proj_load.wait()
    slab = jnp.where(c == 0, proj[:, 0, :], proj[:, 1, :])
    slab = lax.dot_general(order, slab, (((0,), (1,)), ((), ())), preferred_element_type=F32).astype(BF16)
    for h in range(2):
        pfull[h, :, own_lanes] = slab[h * half_rank : (h + 1) * half_rank]
    pl.semaphore_wait(barrier, len(greeted))
    for peer in relays:
        pl.semaphore_signal(line_sem, inc=1, device_id=peer, device_id_type=MESH)

    def p_copy(h, src, first, count, recv, peer):
        at = pl.ds(pl.multiple_of(src * rows, rows), rows)
        ref = pfull.at[h, pl.ds(first, count), at]
        return pltpu.make_async_remote_copy(ref, ref, p_send.at[h], recv, device_id=peer, device_id_type=MESH)

    hr = half_rank // 2

    def p_first(h):
        for d in axis_offsets:
            p_copy(h, fs, 0, half_rank, pf_recv.at[h, axis_offsets.index(d)], fs_peer(d)).start()

    def p_onward(h, k):
        if k < NX:
            p_copy(h, fs_source(k), 0, half_rank, pf_recv.at[h, axis_offsets.index(k)], fs_peer(k)).wait_recv()
            for j in y_offsets:
                p_copy(h, fs_source(k), 0, hr, pd_recv.at[h, j], fs_peer(j * NX)).start()
        if k < NY:
            sem = pf_recv.at[h, axis_offsets.index(k * NX)]
            p_copy(h, fs_source(k * NX), 0, half_rank, sem, fs_peer(k * NX)).wait_recv()
            for j in x_offsets:
                p_copy(h, fs_source(k * NX), hr, hr, pd_recv.at[h, k], fs_peer(j)).start()

    moment_copies = tuple(
        pltpu.make_async_remote_copy(
            src, dst.at[0], moment_send.at[i], moment_recv.at[i], device_id=partner, device_id_type=MESH
        )
        for i, (src, dst) in enumerate(((fm_hbm, fm), (sm_hbm, sm)))
    )

    p_first(0)

    @pl.when(c == 0)
    def _():
        for copy in swaps(b_hbm, cv_hbm) + moment_copies:
            copy.start()

    @pl.when(c == 1)
    def _():
        for copy in swaps(x_hbm, g_hbm):
            copy.start()

    steps = sorted(range(1, max(NX, NY)), key=lambda k: hops(k, max(NX, NY)))
    p_first(1)
    for h in range(2):
        for k in steps:
            p_onward(h, k)

    for copy in own_loads(x_hbm, g_hbm):
        copy.wait()
    for copy in swaps(x_hbm, g_hbm):
        copy.wait_recv()

    def rs_copy(h, d, dst):
        return pltpu.make_async_remote_copy(
            lowb.at[h, dst], rs.at[h, d], rs_send.at[h], rs_recv.at[h], device_id=fs_peer(d), device_id_type=MESH
        )

    def fs_target(d):
        return lax.rem(y + d // NX, NY) * NX + lax.rem(x + d % NX, NX)

    across = (((1,), (1,)), ((), ()))

    def mix_slabs(h, dy):
        if dy > 0:
            arrived(pfull.at[h, :, pl.ds(0, (NX - 1) * rows)], pd_recv.at[h, dy])
        ydim = lax.rem(y + NY - dy, NY)
        at = pl.ds(pl.multiple_of(ydim * (NX * rows), NX * rows), NX * rows)
        for s in range(2):
            term = lax.dot_general(pfull[h, :, at], ax[s, :, at], across, preferred_element_type=F32)
            span = slice(s * tokens, (s + 1) * tokens)
            if dy == 0:
                mix[h, :, span] = term
            else:
                mix[h, :, span] += term

    for h in range(2):
        mix_slabs(h, 0)
    cots = ag[...].reshape(2 * tokens, ag.shape[-1])
    for h in range(2):
        for dy in range(1, NY):
            mix_slabs(h, dy)

        both = mix[h]
        upper = both.astype(BF16)
        lower = (both - upper.astype(F32)).astype(BF16)
        pair = jnp.dot(jnp.concatenate([upper, lower], axis=0), cots, preferred_element_type=F32)
        part = pair[:half_rank] + pair[half_rank:]
        low[h] = part.reshape(NFS, hk, part.shape[-1])
        lowb[h] = low[h].astype(BF16)
        for d in fs_offsets:
            rs_copy(h, d, fs_target(d)).start()

    po_copy = pltpu.make_async_remote_copy(
        pfull, pfull, po_sem.at[0], po_sem.at[1], device_id=partner, device_id_type=MESH
    )
    po_copy.start()

    for copy in late_loads:
        copy.wait()

    def m_copy(m, src, send, recv, peer):
        at = pl.ds(pl.multiple_of(src * rows, rows), rows)
        return pltpu.make_async_remote_copy(
            masters.at[m, :, at], masters.at[m, :, at], send, recv, device_id=peer, device_id_type=MESH
        )

    def m_first():
        for d in axis_offsets:
            for m in range(2):
                m_copy(m, fs, mf_send, mf_recv, fs_peer(d)).start()

    pl.when(c == 0)(m_first)

    sums = []
    for h in range(2):
        total = low[h, fs]
        arrived(rs.at[h, pl.ds(1, NFS - 1)], rs_recv.at[h])
        for d in range(1, NFS):
            total = total + rs[h, d].astype(F32)
        sums.append(total)
    for h in range(2):
        psf[h] = sums[h]
        psb[h] = sums[h].astype(BF16)

    def z_copy(dz):
        zt = lax.rem(z + dz, NZ)
        return pltpu.make_async_remote_copy(
            psb.at[:, :, pl.ds(pl.multiple_of(zt * width, width), width)],
            zb.at[2 * dz + c],
            z_send,
            z_recv,
            device_id=(y, x, zt, 1),
            device_id_type=MESH,
        )

    pl.semaphore_wait(line_sem, len(relays))
    for dz in z_offsets:
        z_copy(dz).start()
    pl.when(c == 0)(lambda: z_copy(0).start())

    pl.when(c == 1)(m_first)

    def d_copy(d):
        at = pl.ds(pl.multiple_of(fs * rk, rk), rk)
        return pltpu.make_async_remote_copy(
            dall.at[:, at], dall.at[:, at], d_send, d_recv, device_id=fs_peer(d), device_id_type=MESH
        )

    back_copies = (
        pltpu.make_async_remote_copy(
            fx.at[0], fx.at[0], back_sem.at[0], back_sem.at[1], device_id=partner, device_id_type=MESH
        ),
        pltpu.make_async_remote_copy(
            dall, dall, back_sem.at[2], back_sem.at[3], device_id=partner, device_id_type=MESH
        ),
    )

    def m_onward():
        arrived(masters.at[:, :, pl.ds(0, len(axis_offsets) * rows)], mf_recv)
        for k in range(1, NX):
            for j in y_offsets:
                m_copy(0, fs_source(k), md_send, md_recv, fs_peer(j * NX)).start()
        for k in range(1, NY):
            for j in x_offsets:
                m_copy(1, fs_source(k * NX), md_send, md_recv, fs_peer(j)).start()

    pl.when(c == 0)(m_onward)

    @pl.when(c == 1)
    def _():
        for copy in moment_copies:
            copy.wait_recv()
        arrived(zb.at[pl.ds(0, 2 * NZ - 1)], z_recv)
        wholes = [zb[0].astype(F32), psf[:, :, pl.ds(pl.multiple_of(z * width, width), width)]]
        for dz in range(1, NZ):
            for m in range(2):
                wholes[m] = wholes[m] + zb[2 * dz + m].astype(F32)
        for m in range(2):
            part = wholes[m].reshape(rk, width)
            first_in = jnp.concatenate([fm[0, :, m, :], fm[1, :, m, :]], axis=1)
            second_in = jnp.concatenate([sm[0, :, m, :], sm[1, :, m, :]], axis=1)
            first = BETA_FIRST * first_in + (1.0 - BETA_FIRST) * part
            second = BETA_SECOND * second_in + (1.0 - BETA_SECOND) * part * part
            dall[m, pl.ds(pl.multiple_of(fs * rk, rk), rk), :] = (first / jnp.sqrt(second)).astype(BF16)
            for i in range(2):
                fx[i, 0, :, m, :] = first[:, i * half : (i + 1) * half]
                fx[i, 1, :, m, :] = second[:, i * half : (i + 1) * half]
        for d in fs_offsets:
            d_copy(d).start()
        back_copies[0].start()

    pl.when(c == 1)(m_onward)

    def c_copy(dz, core):
        return pltpu.make_async_remote_copy(
            cb.at[0],
            cb.at[dz],
            c_send,
            c_recv,
            device_id=(y, x, lax.rem(z + dz, NZ), core),
            device_id_type=MESH,
        )

    @pl.when(c == 1)
    def _():
        arrived(dall.at[:, pl.ds(0, (NFS - 1) * rk)], d_recv)
        for m in range(2):
            wide = dall[m].astype(F32)
            cb[0, pl.ds(m, 1), :] = jnp.sum(wide * wide, axis=0, keepdims=True)
        for dz in z_offsets:
            for core in range(2):
                c_copy(dz, core).start()
        c_copy(0, 0).start()
        back_copies[1].start()

    pl.when(c == 0)(lambda: back_copies[1].wait_recv())

    po_copy.wait_recv()
    for m in range(2):
        turned = lax.dot_general(
            dall[m], order, (((0,), (0,)), ((), ())), preferred_element_type=F32
        ).astype(BF16)
        raws[m] = jnp.dot(
            jnp.where(c == 0, turned[:half], turned[half:]),
            pboth[m].reshape(rank, pboth.shape[-1]),
            preferred_element_type=F32,
        )

    pl.when(c == 0)(lambda: arrived(cb.at[pl.ds(0, NZ)], c_recv))
    pl.when(c == 1)(lambda: arrived(cb.at[pl.ds(1, NZ - 1)], c_recv))
    squares = cb[0]
    for dz in range(1, NZ):
        squares = squares + cb[dz]
    clip_level = CLIP_SHARE * math.sqrt(rank * width * NZ)
    factors = []
    for m in range(2):
        norm = jnp.sqrt(jnp.sum(squares[m : m + 1], axis=(0, 1), keepdims=True))
        factors.append(clip_level / jnp.maximum(norm, clip_level))
    steps = (sg_out, so_out)
    news = (gn_out, on_out)
    for m in range(2):
        step = raws[m, :, own_lanes] * factors[m]
        steps[m][...] = step
        news[m][...] = masters[m, :, own_lanes] - LEARN_RATE * step
    diagonal = (NY - 1) * (NX - 1)
    arrived(masters.at[:, :, pl.ds(0, diagonal * rows)], md_recv)
    for m in range(2):
        ebuf[m] = (masters[m] - LEARN_RATE * (raws[m] * factors[m])).astype(BF16)

    for h in range(2):
        arrived(pfull.at[h, :, pl.ds(0, (NFS - 1) * rows)], p_send.at[h])
        arrived(rs.at[h, pl.ds(1, NFS - 1)], rs_send.at[h])
    po_copy.wait_send()
    arrived(masters.at[:, :, pl.ds(0, len(axis_offsets) * rows)], mf_send)
    arrived(masters.at[:, :, pl.ds(0, diagonal * rows)], md_send)

    @pl.when(c == 0)
    def _():
        arrived(zb.at[pl.ds(0, NZ)], z_send)
        for copy in moment_copies:
            copy.wait_send()
        back_copies[0].wait_recv()

    @pl.when(c == 1)
    def _():
        arrived(zb.at[pl.ds(0, NZ - 1)], z_send)
        arrived(dall.at[:, pl.ds(0, (NFS - 1) * rk)], d_send)
        arrived(cb.at[pl.ds(0, 2 * NZ - 1)], c_send)
        for copy in back_copies:
            copy.wait_send()

    fn_out[...] = fx[c, 0]
    sn_out[...] = fx[c, 1]
    for copy in swaps(x_hbm, g_hbm):
        copy.wait_send()


def store_kernel(*refs):
    count = (len(refs) - 2) // 2
    ins, outs, sem = refs[:count], refs[count:-1], refs[-1]
    sources = [*ins[:-1], ins[-1].at[0], ins[-1].at[1]]
    copies = [pltpu.make_async_copy(src, dst, sem.at[i]) for i, (src, dst) in enumerate(zip(sources, outs))]
    for copy in copies:
        copy.start()
    for copy in copies:
        copy.wait()


def shards(sizes, x, g, cv, b, proj, fm, sm, gm, om):
    NY, NX, NZ = sizes
    NFS = NY * NX
    tokens, d_model = x.shape
    channels = g.shape[1]
    rows, _, rank = proj.shape
    rk = rank // NFS
    cols = gm.shape[1]
    width = 2 * cols
    vmem = pl.BlockSpec(memory_space=pltpu.VMEM)
    hbm = pl.BlockSpec(memory_space=pltpu.HBM)
    dma = pltpu.SemaphoreType.DMA
    small = jax.ShapeDtypeStruct(fm.shape, F32)
    block = jax.ShapeDtypeStruct((cols, rows), F32)
    copy = jax.ShapeDtypeStruct((cols, d_model), BF16)
    results = pl.pallas_call(
        functools.partial(kernel, sizes),
        out_shape=(small, small, block, block, block, block, jax.ShapeDtypeStruct((2, cols, d_model), BF16)),
        in_specs=[hbm] * 9,
        out_specs=(vmem,) * 7,
        scratch_shapes=[
            pltpu.VMEM(proj.shape, BF16),
            pltpu.VMEM((2, *fm.shape), F32),
            pltpu.VMEM((2, *sm.shape), F32),
            pltpu.VMEM((2, tokens, d_model), BF16),
            pltpu.VMEM((2, tokens, channels), BF16),
            pltpu.VMEM((2, 2, rank // 2, d_model), BF16),
            pltpu.VMEM((2, cols, d_model), F32),
            pltpu.VMEM((2, cols, d_model), F32),
            pltpu.VMEM((2, rank // 2, 2 * tokens), F32),
            pltpu.VMEM((2, NFS, rk // 2, channels), F32),
            pltpu.VMEM((2, NFS, rk // 2, channels), BF16),
            pltpu.VMEM((2, NFS, rk // 2, channels), BF16),
            pltpu.VMEM((2, rk // 2, channels), F32),
            pltpu.VMEM((2, rk // 2, channels), BF16),
            pltpu.VMEM((2 * NZ, 2, rk // 2, width), BF16),
            pltpu.VMEM((2, rank, width), BF16),
            pltpu.VMEM((2 * NZ, 2, width), F32),
            pltpu.VMEM((2, 2, *fm.shape), F32),
            dma((7,)),
            dma((2,)),
            dma((2,)),
        ]
        + [dma((2,)), dma((2, NX + NY - 2)), dma((2, NY))]
        + [dma((2,))] * 2
        + [dma] * 6
        + [dma((2,))]
        + [dma] * 4
        + [pltpu.SemaphoreType.REGULAR]
        + [dma((2,)), dma((2,)), dma((4,))],
        compiler_params=pltpu.CompilerParams(collective_id=0, has_side_effects=True, vmem_limit_bytes=48 * 2**20),
    )(*(pltpu.with_memory_space_constraint(a, pltpu.HBM) for a in (x, g, cv, b, proj, fm, sm, gm.T, om)))
    fn, sn, sg, so, gn, on, gc, oc = pl.pallas_call(
        store_kernel,
        out_shape=(small, small, block, block, block, block, copy, copy),
        in_specs=[vmem] * 7,
        out_specs=(hbm,) * 8,
        scratch_shapes=[dma((8,))],
        compiler_params=pltpu.CompilerParams(vmem_limit_bytes=2**20),
    )(*results)
    return fn, sn, sg.T, so, gn.T, on, gc.T, oc


def solution(mesh):
    sizes = (4, 4, 8)
    split = Mesh(mesh.devices.reshape(*sizes, 2), FS_TP)
    return build(split, sizes)


def build(split, sizes):
    in_specs = (
        P(FS_TP, None),
        P(FS_TP, None),
        P(FS_TP, None),
        P(FS_TP, None),
        P(FS, None, None),
        P(FS, None, TP),
        P(FS, None, TP),
        P(FS, TP),
        P(TP, FS),
    )
    out_specs = (
        P(FS, None, TP),
        P(FS, None, TP),
        P(FS, TP),
        P(TP, FS),
        P(FS, TP),
        P(TP, FS),
        P(None, TP),
        P(TP, None),
    )
    return jax.shard_map(
        functools.partial(shards, sizes), mesh=split, in_specs=in_specs, out_specs=out_specs, check_vma=False
    )
```

```python
import functools
import math

import jax
import jax.numpy as jnp
from jax import lax
from jax.experimental import pallas as pl
from jax.experimental.pallas import tpu as pltpu
from jax.sharding import Mesh
from jax.sharding import PartitionSpec as P

MESH = pl.DeviceIdType.MESH
F32 = jnp.float32
BF16 = jnp.bfloat16
FS = ("y", "x")
TP = ("z", "c")
FS_TP = ("y", "x", "z", "c")

BETA_FIRST = 0.8
BETA_SECOND = 0.9
LEARN_RATE = 0.01
CLIP_SHARE = 0.5


def kernel(
    sizes,
    x_hbm,
    g_hbm,
    cv_hbm,
    b_hbm,
    proj_hbm,
    fm_hbm,
    sm_hbm,
    gm_hbm,
    om_hbm,
    fn_out,
    sn_out,
    sg_out,
    so_out,
    gn_out,
    on_out,
    ebuf,
    proj,
    fm,
    sm,
    ax,
    ag,
    pboth,
    masters,
    raws,
    mix,
    low,
    lowb,
    rs,
    psf,
    psb,
    zb,
    dall,
    cb,
    fx,
    load_sem,
    swap_send,
    swap_recv,
    p_send,
    pf_recv,
    pd_recv,
    rs_send,
    rs_recv,
    z_send,
    z_recv,
    d_send,
    d_recv,
    c_send,
    c_recv,
    po_sem,
    mf_send,
    mf_recv,
    md_send,
    md_recv,
    line_sem,
    moment_send,
    moment_recv,
    back_sem,
):
    NY, NX, NZ = sizes
    NFS = NY * NX
    tokens = x_hbm.shape[0]
    rows = proj.shape[0]
    rank = 2 * pboth.shape[2]
    rk = rank // NFS
    width = zb.shape[-1]
    half = width // 2
    y, x = lax.axis_index("y"), lax.axis_index("x")
    z, c = lax.axis_index("z"), lax.axis_index("c")
    fs = y * NX + x
    pfull = pboth.at[c]
    own = pl.multiple_of(fs * rows, rows)
    own_lanes = pl.ds(own, rows)

    def fs_peer(d):
        return (lax.rem(y + d // NX, NY), lax.rem(x + d % NX, NX), z, c)

    def fs_source(d):
        return lax.rem(y + NY - d // NX, NY) * NX + lax.rem(x + NX - d % NX, NX)

    def tp_peer(e):
        return (y, x, lax.rem(z + e // 2, NZ), lax.rem(c + e % 2, 2))

    partner = (y, x, z, 1 - c)

    def hops(k, n):
        return min(k, n - k)

    fs_offsets = sorted(range(1, NFS), key=lambda d: -hops(d // NX, NY) - hops(d % NX, NX))
    z_offsets = sorted(range(1, NZ), key=lambda k: -hops(k, NZ))
    y_offsets = sorted(range(1, NY), key=lambda j: -hops(j, NY))
    x_offsets = sorted(range(1, NX), key=lambda j: -hops(j, NX))

    def own_loads(act, cot):
        return (
            pltpu.make_async_copy(act, ax.at[0], load_sem.at[0]),
            pltpu.make_async_copy(cot, ag.at[0], load_sem.at[1]),
        )

    def swaps(act, cot):
        return (
            pltpu.make_async_remote_copy(
                act, ax.at[1], swap_send.at[0], swap_recv.at[0], device_id=partner, device_id_type=MESH
            ),
            pltpu.make_async_remote_copy(
                cot, ag.at[1], swap_send.at[1], swap_recv.at[1], device_id=partner, device_id_type=MESH
            ),
        )

    proj_load = pltpu.make_async_copy(proj_hbm, proj, load_sem.at[2])
    proj_load.start()
    axis_offsets = [k for k in range(1, NX)] + [k * NX for k in range(1, NY)]
    near = [k for k in range(1, NZ) if hops(k, NZ) <= 2]
    relays = [(y, x, lax.rem(z + k, NZ), c) for k in near if hops(k, NZ) == 2]
    greeted = [fs_peer(d) for d in axis_offsets] + [partner] + [tp_peer(2 * k + i) for k in near for i in range(2)]
    barrier = pltpu.get_barrier_semaphore()
    for peer in greeted:
        pl.semaphore_signal(barrier, inc=1, device_id=peer, device_id_type=MESH)

    @pl.when(c == 0)
    def _():
        for copy in own_loads(x_hbm, g_hbm):
            copy.start()

    @pl.when(c == 1)
    def _():
        for copy in own_loads(b_hbm, cv_hbm):
            copy.start()

    late_loads = [
        pltpu.make_async_copy(src, dst, load_sem.at[3 + i])
        for i, (src, dst) in enumerate(
            ((fm_hbm, fm.at[c]), (sm_hbm, sm.at[c]), (gm_hbm, masters.at[0, :, own_lanes]), (om_hbm, masters.at[1, :, own_lanes]))
        )
    ]
    for copy in late_loads:
        copy.start()

    def arrived(like, sem):
        pltpu.make_async_copy(like, like, sem).wait()

    hk, half_rank = rk // 2, rank // 2
    natural = lax.broadcasted_iota(jnp.int32, (rank, rank), 0)
    place = lax.broadcasted_iota(jnp.int32, (rank, rank), 1)
    inner = lax.rem(place, half_rank)
    wanted = lax.div(inner, hk) * rk + lax.div(place, half_rank) * hk + lax.rem(inner, hk)
    order = jnp.where(natural == wanted, 1.0, 0.0).astype(BF16)
    proj_load.wait()
    slab = jnp.where(c == 0, proj[:, 0, :], proj[:, 1, :])
    slab = lax.dot_general(order, slab, (((0,), (1,)), ((), ())), preferred_element_type=F32).astype(BF16)
    for h in range(2):
        pfull[h, :, own_lanes] = slab[h * half_rank : (h + 1) * half_rank]
    pl.semaphore_wait(barrier, len(greeted))
    for peer in relays:
        pl.semaphore_signal(line_sem, inc=1, device_id=peer, device_id_type=MESH)

    def p_copy(h, src, first, count, recv, peer):
        at = pl.ds(pl.multiple_of(src * rows, rows), rows)
        ref = pfull.at[h, pl.ds(first, count), at]
        return pltpu.make_async_remote_copy(ref, ref, p_send.at[h], recv, device_id=peer, device_id_type=MESH)

    hr = half_rank // 2

    def p_first(h):
        for d in axis_offsets:
            p_copy(h, fs, 0, half_rank, pf_recv.at[h, axis_offsets.index(d)], fs_peer(d)).start()

    def p_onward(h, k):
        if k < NX:
            p_copy(h, fs_source(k), 0, half_rank, pf_recv.at[h, axis_offsets.index(k)], fs_peer(k)).wait_recv()
            for j in y_offsets:
                p_copy(h, fs_source(k), 0, hr, pd_recv.at[h, j], fs_peer(j * NX)).start()
        if k < NY:
            sem = pf_recv.at[h, axis_offsets.index(k * NX)]
            p_copy(h, fs_source(k * NX), 0, half_rank, sem, fs_peer(k * NX)).wait_recv()
            for j in x_offsets:
                p_copy(h, fs_source(k * NX), hr, hr, pd_recv.at[h, k], fs_peer(j)).start()

    moment_copies = tuple(
        pltpu.make_async_remote_copy(
            src, dst.at[0], moment_send.at[i], moment_recv.at[i], device_id=partner, device_id_type=MESH
        )
        for i, (src, dst) in enumerate(((fm_hbm, fm), (sm_hbm, sm)))
    )

    p_first(0)

    @pl.when(c == 0)
    def _():
        for copy in swaps(b_hbm, cv_hbm) + moment_copies:
            copy.start()

    @pl.when(c == 1)
    def _():
        for copy in swaps(x_hbm, g_hbm):
            copy.start()

    steps = sorted(range(1, max(NX, NY)), key=lambda k: hops(k, max(NX, NY)))
    p_first(1)
    for h in range(2):
        for k in steps:
            p_onward(h, k)

    for copy in own_loads(x_hbm, g_hbm):
        copy.wait()
    for copy in swaps(x_hbm, g_hbm):
        copy.wait_recv()

    def rs_copy(h, d):
        return pltpu.make_async_remote_copy(
            lowb.at[h, fs_target(d)],
            rs.at[c, h, d],
            rs_send.at[h],
            rs_recv.at[c, h],
            device_id=(*fs_peer(d)[:2], z, 1),
            device_id_type=MESH,
        )

    def fs_target(d):
        return lax.rem(y + d // NX, NY) * NX + lax.rem(x + d % NX, NX)

    across = (((1,), (1,)), ((), ()))

    def mix_slabs(h, dy):
        if dy > 0:
            arrived(pfull.at[h, :, pl.ds(0, (NX - 1) * rows)], pd_recv.at[h, dy])
        ydim = lax.rem(y + NY - dy, NY)
        at = pl.ds(pl.multiple_of(ydim * (NX * rows), NX * rows), NX * rows)
        for s in range(2):
            term = lax.dot_general(pfull[h, :, at], ax[s, :, at], across, preferred_element_type=F32)
            span = slice(s * tokens, (s + 1) * tokens)
            if dy == 0:
                mix[h, :, span] = term
            else:
                mix[h, :, span] += term

    for h in range(2):
        mix_slabs(h, 0)
    cots = ag[...].reshape(2 * tokens, ag.shape[-1])
    for h in range(2):
        for dy in range(1, NY):
            mix_slabs(h, dy)

        both = mix[h]
        upper = both.astype(BF16)
        lower = (both - upper.astype(F32)).astype(BF16)
        pair = jnp.dot(jnp.concatenate([upper, lower], axis=0), cots, preferred_element_type=F32)
        part = pair[:half_rank] + pair[half_rank:]
        low[h] = part.reshape(NFS, hk, part.shape[-1])
        lowb[h] = low[h].astype(BF16)
        for d in fs_offsets:
            rs_copy(h, d).start()
        pl.when(c == 0)(lambda: rs_copy(h, 0).start())

    po_copy = pltpu.make_async_remote_copy(
        pfull, pfull, po_sem.at[0], po_sem.at[1], device_id=partner, device_id_type=MESH
    )
    po_copy.start()

    for copy in late_loads:
        copy.wait()

    def m_copy(m, src, send, recv, peer):
        at = pl.ds(pl.multiple_of(src * rows, rows), rows)
        return pltpu.make_async_remote_copy(
            masters.at[m, :, at], masters.at[m, :, at], send, recv, device_id=peer, device_id_type=MESH
        )

    def m_first():
        for d in axis_offsets:
            for m in range(2):
                m_copy(m, fs, mf_send, mf_recv, fs_peer(d)).start()

    pl.when(c == 0)(m_first)

    @pl.when(c == 1)
    def _():
        for m in (1, 0):
            for h in range(2):
                arrived(rs.at[m, h, pl.ds(m, NFS - m)], rs_recv.at[m, h])
                total = low[h, fs] if m else rs[0, h, 0].astype(F32)
                for d in range(1, NFS):
                    total = total + rs[m, h, d].astype(F32)
                psf[m, h] = total
                psb[m, h] = total.astype(BF16)

    def z_copy(dz):
        zt = lax.rem(z + dz, NZ)
        return pltpu.make_async_remote_copy(
            psb.at[:, :, :, pl.ds(pl.multiple_of(zt * width, width), width)],
            zb.at[dz],
            z_send,
            z_recv,
            device_id=(y, x, zt, 1),
            device_id_type=MESH,
        )

    pl.semaphore_wait(line_sem, len(relays))

    @pl.when(c == 1)
    def _():
        for dz in z_offsets:
            z_copy(dz).start()
        m_first()

    def d_copy(d):
        at = pl.ds(pl.multiple_of(fs * rk, rk), rk)
        return pltpu.make_async_remote_copy(
            dall.at[:, at], dall.at[:, at], d_send, d_recv, device_id=fs_peer(d), device_id_type=MESH
        )

    back_copies = (
        pltpu.make_async_remote_copy(
            fx.at[0], fx.at[0], back_sem.at[0], back_sem.at[1], device_id=partner, device_id_type=MESH
        ),
        pltpu.make_async_remote_copy(
            dall, dall, back_sem.at[2], back_sem.at[3], device_id=partner, device_id_type=MESH
        ),
    )

    def m_onward():
        arrived(masters.at[:, :, pl.ds(0, len(axis_offsets) * rows)], mf_recv)
        for k in range(1, NX):
            for j in y_offsets:
                m_copy(0, fs_source(k), md_send, md_recv, fs_peer(j * NX)).start()
        for k in range(1, NY):
            for j in x_offsets:
                m_copy(1, fs_source(k * NX), md_send, md_recv, fs_peer(j)).start()

    pl.when(c == 0)(m_onward)

    @pl.when(c == 1)
    def _():
        for copy in moment_copies:
            copy.wait_recv()
        arrived(zb.at[pl.ds(1, NZ - 1)], z_recv)
        wholes = [psf[m, :, :, pl.ds(pl.multiple_of(z * width, width), width)] for m in range(2)]
        for dz in range(1, NZ):
            for m in range(2):
                wholes[m] = wholes[m] + zb[dz, m].astype(F32)
        for m in range(2):
            part = wholes[m].reshape(rk, width)
            first_in = jnp.concatenate([fm[0, :, m, :], fm[1, :, m, :]], axis=1)
            second_in = jnp.concatenate([sm[0, :, m, :], sm[1, :, m, :]], axis=1)
            first = BETA_FIRST * first_in + (1.0 - BETA_FIRST) * part
            second = BETA_SECOND * second_in + (1.0 - BETA_SECOND) * part * part
            dall[m, pl.ds(pl.multiple_of(fs * rk, rk), rk), :] = (first / jnp.sqrt(second)).astype(BF16)
            for i in range(2):
                fx[i, 0, :, m, :] = first[:, i * half : (i + 1) * half]
                fx[i, 1, :, m, :] = second[:, i * half : (i + 1) * half]
        for d in fs_offsets:
            d_copy(d).start()
        back_copies[0].start()

    pl.when(c == 1)(m_onward)

    def c_copy(dz, core):
        return pltpu.make_async_remote_copy(
            cb.at[0],
            cb.at[dz],
            c_send,
            c_recv,
            device_id=(y, x, lax.rem(z + dz, NZ), core),
            device_id_type=MESH,
        )

    @pl.when(c == 1)
    def _():
        arrived(dall.at[:, pl.ds(0, (NFS - 1) * rk)], d_recv)
        for m in range(2):
            wide = dall[m].astype(F32)
            cb[0, pl.ds(m, 1), :] = jnp.sum(wide * wide, axis=0, keepdims=True)
        for dz in z_offsets:
            for core in range(2):
                c_copy(dz, core).start()
        c_copy(0, 0).start()
        back_copies[1].start()

    pl.when(c == 0)(lambda: back_copies[1].wait_recv())

    po_copy.wait_recv()
    for m in range(2):
        turned = lax.dot_general(
            dall[m], order, (((0,), (0,)), ((), ())), preferred_element_type=F32
        ).astype(BF16)
        raws[m] = jnp.dot(
            jnp.where(c == 0, turned[:half], turned[half:]),
            pboth[m].reshape(rank, pboth.shape[-1]),
            preferred_element_type=F32,
        )

    pl.when(c == 0)(lambda: arrived(cb.at[pl.ds(0, NZ)], c_recv))
    pl.when(c == 1)(lambda: arrived(cb.at[pl.ds(1, NZ - 1)], c_recv))
    squares = cb[0]
    for dz in range(1, NZ):
        squares = squares + cb[dz]
    clip_level = CLIP_SHARE * math.sqrt(rank * width * NZ)
    factors = []
    for m in range(2):
        norm = jnp.sqrt(jnp.sum(squares[m : m + 1], axis=(0, 1), keepdims=True))
        factors.append(clip_level / jnp.maximum(norm, clip_level))
    steps = (sg_out, so_out)
    news = (gn_out, on_out)
    for m in range(2):
        step = raws[m, :, own_lanes] * factors[m]
        steps[m][...] = step
        news[m][...] = masters[m, :, own_lanes] - LEARN_RATE * step
    diagonal = (NY - 1) * (NX - 1)
    arrived(masters.at[:, :, pl.ds(0, diagonal * rows)], md_recv)
    for m in range(2):
        ebuf[m] = (masters[m] - LEARN_RATE * (raws[m] * factors[m])).astype(BF16)

    for h in range(2):
        arrived(pfull.at[h, :, pl.ds(0, (NFS - 1) * rows)], p_send.at[h])
    po_copy.wait_send()
    arrived(masters.at[:, :, pl.ds(0, len(axis_offsets) * rows)], mf_send)
    arrived(masters.at[:, :, pl.ds(0, diagonal * rows)], md_send)

    @pl.when(c == 0)
    def _():
        for h in range(2):
            arrived(rs.at[0, h], rs_send.at[h])
        for copy in moment_copies:
            copy.wait_send()
        back_copies[0].wait_recv()

    @pl.when(c == 1)
    def _():
        for h in range(2):
            arrived(rs.at[0, h, pl.ds(0, NFS - 1)], rs_send.at[h])
        arrived(zb.at[pl.ds(0, NZ - 1)], z_send)
        arrived(dall.at[:, pl.ds(0, (NFS - 1) * rk)], d_send)
        arrived(cb.at[pl.ds(0, 2 * NZ - 1)], c_send)
        for copy in back_copies:
            copy.wait_send()

    fn_out[...] = fx[c, 0]
    sn_out[...] = fx[c, 1]
    for copy in swaps(x_hbm, g_hbm):
        copy.wait_send()


def store_kernel(*refs):
    count = (len(refs) - 2) // 2
    ins, outs, sem = refs[:count], refs[count:-1], refs[-1]
    sources = [*ins[:-1], ins[-1].at[0], ins[-1].at[1]]
    copies = [pltpu.make_async_copy(src, dst, sem.at[i]) for i, (src, dst) in enumerate(zip(sources, outs))]
    for copy in copies:
        copy.start()
    for copy in copies:
        copy.wait()


def shards(sizes, x, g, cv, b, proj, fm, sm, gm, om):
    NY, NX, NZ = sizes
    NFS = NY * NX
    tokens, d_model = x.shape
    channels = g.shape[1]
    rows, _, rank = proj.shape
    rk = rank // NFS
    cols = gm.shape[1]
    width = 2 * cols
    vmem = pl.BlockSpec(memory_space=pltpu.VMEM)
    hbm = pl.BlockSpec(memory_space=pltpu.HBM)
    dma = pltpu.SemaphoreType.DMA
    small = jax.ShapeDtypeStruct(fm.shape, F32)
    block = jax.ShapeDtypeStruct((cols, rows), F32)
    copy = jax.ShapeDtypeStruct((cols, d_model), BF16)
    results = pl.pallas_call(
        functools.partial(kernel, sizes),
        out_shape=(small, small, block, block, block, block, jax.ShapeDtypeStruct((2, cols, d_model), BF16)),
        in_specs=[hbm] * 9,
        out_specs=(vmem,) * 7,
        scratch_shapes=[
            pltpu.VMEM(proj.shape, BF16),
            pltpu.VMEM((2, *fm.shape), F32),
            pltpu.VMEM((2, *sm.shape), F32),
            pltpu.VMEM((2, tokens, d_model), BF16),
            pltpu.VMEM((2, tokens, channels), BF16),
            pltpu.VMEM((2, 2, rank // 2, d_model), BF16),
            pltpu.VMEM((2, cols, d_model), F32),
            pltpu.VMEM((2, cols, d_model), F32),
            pltpu.VMEM((2, rank // 2, 2 * tokens), F32),
            pltpu.VMEM((2, NFS, rk // 2, channels), F32),
            pltpu.VMEM((2, NFS, rk // 2, channels), BF16),
            pltpu.VMEM((2, 2, NFS, rk // 2, channels), BF16),
            pltpu.VMEM((2, 2, rk // 2, channels), F32),
            pltpu.VMEM((2, 2, rk // 2, channels), BF16),
            pltpu.VMEM((NZ, 2, 2, rk // 2, width), BF16),
            pltpu.VMEM((2, rank, width), BF16),
            pltpu.VMEM((2 * NZ, 2, width), F32),
            pltpu.VMEM((2, 2, *fm.shape), F32),
            dma((7,)),
            dma((2,)),
            dma((2,)),
        ]
        + [dma((2,)), dma((2, NX + NY - 2)), dma((2, NY))]
        + [dma((2,)), dma((2, 2))]
        + [dma] * 6
        + [dma((2,))]
        + [dma] * 4
        + [pltpu.SemaphoreType.REGULAR]
        + [dma((2,)), dma((2,)), dma((4,))],
        compiler_params=pltpu.CompilerParams(collective_id=0, has_side_effects=True, vmem_limit_bytes=48 * 2**20),
    )(*(pltpu.with_memory_space_constraint(a, pltpu.HBM) for a in (x, g, cv, b, proj, fm, sm, gm.T, om)))
    fn, sn, sg, so, gn, on, gc, oc = pl.pallas_call(
        store_kernel,
        out_shape=(small, small, block, block, block, block, copy, copy),
        in_specs=[vmem] * 7,
        out_specs=(hbm,) * 8,
        scratch_shapes=[dma((8,))],
        compiler_params=pltpu.CompilerParams(vmem_limit_bytes=2**20),
    )(*results)
    return fn, sn, sg.T, so, gn.T, on, gc.T, oc


def solution(mesh):
    sizes = (4, 4, 8)
    split = Mesh(mesh.devices.reshape(*sizes, 2), FS_TP)
    return build(split, sizes)


def build(split, sizes):
    in_specs = (
        P(FS_TP, None),
        P(FS_TP, None),
        P(FS_TP, None),
        P(FS_TP, None),
        P(FS, None, None),
        P(FS, None, TP),
        P(FS, None, TP),
        P(FS, TP),
        P(TP, FS),
    )
    out_specs = (
        P(FS, None, TP),
        P(FS, None, TP),
        P(FS, TP),
        P(TP, FS),
        P(FS, TP),
        P(TP, FS),
        P(None, TP),
        P(TP, None),
    )
    return jax.shard_map(
        functools.partial(shards, sizes), mesh=split, in_specs=in_specs, out_specs=out_specs, check_vma=False
    )
```

```python
import functools
import math

import jax
import jax.numpy as jnp
from jax import lax
from jax.experimental import pallas as pl
from jax.experimental.pallas import tpu as pltpu
from jax.sharding import Mesh
from jax.sharding import PartitionSpec as P

MESH = pl.DeviceIdType.MESH
F32 = jnp.float32
BF16 = jnp.bfloat16
FS = ("y", "x")
TP = ("z", "c")
FS_TP = ("y", "x", "z", "c")

BETA_FIRST = 0.8
BETA_SECOND = 0.9
LEARN_RATE = 0.01
CLIP_SHARE = 0.5


def kernel(
    sizes,
    x_hbm,
    g_hbm,
    cv_hbm,
    b_hbm,
    proj_hbm,
    fm_hbm,
    sm_hbm,
    gm_hbm,
    om_hbm,
    fn_out,
    sn_out,
    sg_out,
    so_out,
    gn_out,
    on_out,
    ebuf,
    proj,
    fm,
    sm,
    ax,
    ag,
    pboth,
    masters,
    raws,
    mix,
    low,
    lowb,
    rs,
    psf,
    psb,
    zb,
    dall,
    cb,
    fx,
    load_sem,
    swap_send,
    swap_recv,
    p_send,
    pf_recv,
    pd_recv,
    rs_send,
    rs_recv,
    z_send,
    z_recv,
    d_send,
    d_recv,
    c_send,
    c_recv,
    po_sem,
    mf_send,
    mf_recv,
    md_send,
    md_recv,
    line_sem,
    moment_send,
    moment_recv,
    back_sem,
):
    NY, NX, NZ = sizes
    NFS = NY * NX
    tokens = x_hbm.shape[0]
    rows = proj.shape[0]
    rank = 2 * pboth.shape[2]
    rk = rank // NFS
    width = zb.shape[-1]
    half = width // 2
    y, x = lax.axis_index("y"), lax.axis_index("x")
    z, c = lax.axis_index("z"), lax.axis_index("c")
    fs = y * NX + x
    pfull = pboth.at[c]
    own = pl.multiple_of(fs * rows, rows)
    own_lanes = pl.ds(own, rows)

    def fs_peer(d):
        return (lax.rem(y + d // NX, NY), lax.rem(x + d % NX, NX), z, c)

    def fs_source(d):
        return lax.rem(y + NY - d // NX, NY) * NX + lax.rem(x + NX - d % NX, NX)

    def tp_peer(e):
        return (y, x, lax.rem(z + e // 2, NZ), lax.rem(c + e % 2, 2))

    partner = (y, x, z, 1 - c)

    def hops(k, n):
        return min(k, n - k)

    fs_offsets = sorted(range(1, NFS), key=lambda d: -hops(d // NX, NY) - hops(d % NX, NX))
    z_offsets = sorted(range(1, NZ), key=lambda k: -hops(k, NZ))
    y_offsets = sorted(range(1, NY), key=lambda j: -hops(j, NY))
    x_offsets = sorted(range(1, NX), key=lambda j: -hops(j, NX))

    def own_loads(act, cot):
        return (
            pltpu.make_async_copy(act, ax.at[0], load_sem.at[0]),
            pltpu.make_async_copy(cot, ag.at[0], load_sem.at[1]),
        )

    def swaps(act, cot):
        return (
            pltpu.make_async_remote_copy(
                act, ax.at[1], swap_send.at[0], swap_recv.at[0], device_id=partner, device_id_type=MESH
            ),
            pltpu.make_async_remote_copy(
                cot, ag.at[1], swap_send.at[1], swap_recv.at[1], device_id=partner, device_id_type=MESH
            ),
        )

    proj_load = pltpu.make_async_copy(proj_hbm, proj, load_sem.at[2])
    proj_load.start()
    axis_offsets = [k for k in range(1, NX)] + [k * NX for k in range(1, NY)]
    near = [k for k in range(1, NZ) if hops(k, NZ) <= 2]
    relays = [(y, x, lax.rem(z + k, NZ), c) for k in near if hops(k, NZ) == 2]
    greeted = [fs_peer(d) for d in axis_offsets] + [partner] + [tp_peer(2 * k + i) for k in near for i in range(2)]
    barrier = pltpu.get_barrier_semaphore()
    for peer in greeted:
        pl.semaphore_signal(barrier, inc=1, device_id=peer, device_id_type=MESH)

    @pl.when(c == 0)
    def _():
        for copy in own_loads(x_hbm, g_hbm):
            copy.start()

    @pl.when(c == 1)
    def _():
        for copy in own_loads(b_hbm, cv_hbm):
            copy.start()

    late_loads = [
        pltpu.make_async_copy(src, dst, load_sem.at[3 + i])
        for i, (src, dst) in enumerate(
            ((fm_hbm, fm.at[c]), (sm_hbm, sm.at[c]), (gm_hbm, masters.at[0, :, own_lanes]), (om_hbm, masters.at[1, :, own_lanes]))
        )
    ]
    for copy in late_loads:
        copy.start()

    def arrived(like, sem):
        pltpu.make_async_copy(like, like, sem).wait()

    hk, half_rank = rk // 2, rank // 2
    natural = lax.broadcasted_iota(jnp.int32, (rank, rank), 0)
    place = lax.broadcasted_iota(jnp.int32, (rank, rank), 1)
    inner = lax.rem(place, half_rank)
    wanted = lax.div(inner, hk) * rk + lax.div(place, half_rank) * hk + lax.rem(inner, hk)
    order = jnp.where(natural == wanted, 1.0, 0.0).astype(BF16)
    proj_load.wait()
    slab = jnp.where(c == 0, proj[:, 0, :], proj[:, 1, :])
    slab = lax.dot_general(order, slab, (((0,), (1,)), ((), ())), preferred_element_type=F32).astype(BF16)
    for h in range(2):
        pfull[h, :, own_lanes] = slab[h * half_rank : (h + 1) * half_rank]
    pl.semaphore_wait(barrier, len(greeted))
    for peer in relays:
        pl.semaphore_signal(line_sem, inc=1, device_id=peer, device_id_type=MESH)

    def p_copy(h, src, first, count, recv, peer):
        at = pl.ds(pl.multiple_of(src * rows, rows), rows)
        ref = pfull.at[h, pl.ds(first, count), at]
        return pltpu.make_async_remote_copy(ref, ref, p_send.at[h], recv, device_id=peer, device_id_type=MESH)

    hr = half_rank // 2

    def p_first(h):
        for d in axis_offsets:
            p_copy(h, fs, 0, half_rank, pf_recv.at[h, axis_offsets.index(d)], fs_peer(d)).start()

    def p_onward(h, k):
        if k < NX:
            p_copy(h, fs_source(k), 0, half_rank, pf_recv.at[h, axis_offsets.index(k)], fs_peer(k)).wait_recv()
            for j in y_offsets:
                p_copy(h, fs_source(k), 0, hr, pd_recv.at[h, j], fs_peer(j * NX)).start()
        if k < NY:
            sem = pf_recv.at[h, axis_offsets.index(k * NX)]
            p_copy(h, fs_source(k * NX), 0, half_rank, sem, fs_peer(k * NX)).wait_recv()
            for j in x_offsets:
                p_copy(h, fs_source(k * NX), hr, hr, pd_recv.at[h, k], fs_peer(j)).start()

    moment_copies = tuple(
        pltpu.make_async_remote_copy(
            src, dst.at[0], moment_send.at[i], moment_recv.at[i], device_id=partner, device_id_type=MESH
        )
        for i, (src, dst) in enumerate(((fm_hbm, fm), (sm_hbm, sm)))
    )

    p_first(0)

    @pl.when(c == 0)
    def _():
        for copy in swaps(b_hbm, cv_hbm) + moment_copies:
            copy.start()

    @pl.when(c == 1)
    def _():
        for copy in swaps(x_hbm, g_hbm):
            copy.start()

    steps = sorted(range(1, max(NX, NY)), key=lambda k: hops(k, max(NX, NY)))
    p_first(1)
    for h in range(2):
        for k in steps:
            p_onward(h, k)

    for copy in own_loads(x_hbm, g_hbm):
        copy.wait()
    for copy in swaps(x_hbm, g_hbm):
        copy.wait_recv()

    def rs_copy(h, d):
        return pltpu.make_async_remote_copy(
            lowb.at[h, fs_target(d)],
            rs.at[c, h, d],
            rs_send.at[h],
            rs_recv.at[c, h],
            device_id=(*fs_peer(d)[:2], z, 1),
            device_id_type=MESH,
        )

    def fs_target(d):
        return lax.rem(y + d // NX, NY) * NX + lax.rem(x + d % NX, NX)

    across = (((1,), (1,)), ((), ()))

    def mix_slabs(h, dy):
        if dy > 0:
            arrived(pfull.at[h, :, pl.ds(0, (NX - 1) * rows)], pd_recv.at[h, dy])
        ydim = lax.rem(y + NY - dy, NY)
        at = pl.ds(pl.multiple_of(ydim * (NX * rows), NX * rows), NX * rows)
        for s in range(2):
            term = lax.dot_general(pfull[h, :, at], ax[s, :, at], across, preferred_element_type=F32)
            span = slice(s * tokens, (s + 1) * tokens)
            if dy == 0:
                mix[h, :, span] = term
            else:
                mix[h, :, span] += term

    for h in range(2):
        mix_slabs(h, 0)
    cots = ag[...].reshape(2 * tokens, ag.shape[-1])
    for h in range(2):
        for dy in range(1, NY):
            mix_slabs(h, dy)

        both = mix[h]
        upper = both.astype(BF16)
        lower = (both - upper.astype(F32)).astype(BF16)
        pair = jnp.dot(jnp.concatenate([upper, lower], axis=0), cots, preferred_element_type=F32)
        part = pair[:half_rank] + pair[half_rank:]
        low[h] = part.reshape(NFS, hk, part.shape[-1])
        lowb[h] = low[h].astype(BF16)
        for d in fs_offsets:
            rs_copy(h, d).start()
        pl.when(c == 0)(lambda: rs_copy(h, 0).start())

    po_copy = pltpu.make_async_remote_copy(
        pfull, pfull, po_sem.at[0], po_sem.at[1], device_id=partner, device_id_type=MESH
    )
    po_copy.start()

    for copy in late_loads:
        copy.wait()

    def m_copy(m, src, send, recv, peer):
        at = pl.ds(pl.multiple_of(src * rows, rows), rows)
        return pltpu.make_async_remote_copy(
            masters.at[m, :, at], masters.at[m, :, at], send, recv, device_id=peer, device_id_type=MESH
        )

    def m_first():
        for d in axis_offsets:
            for m in range(2):
                m_copy(m, fs, mf_send, mf_recv, fs_peer(d)).start()

    pl.when(c == 0)(m_first)

    @pl.when(c == 1)
    def _():
        for m in (1, 0):
            for h in range(2):
                arrived(rs.at[m, h, pl.ds(m, NFS - m)], rs_recv.at[m, h])
                total = low[h, fs] if m else rs[0, h, 0].astype(F32)
                for d in range(1, NFS):
                    total = total + rs[m, h, d].astype(F32)
                psb[m, h] = total.astype(BF16)
                psf[m, h] = total

    def z_copy(dz):
        zt = lax.rem(z + dz, NZ)
        return pltpu.make_async_remote_copy(
            psb.at[:, :, :, pl.ds(pl.multiple_of(zt * width, width), width)],
            zb.at[dz],
            z_send,
            z_recv,
            device_id=(y, x, zt, 1),
            device_id_type=MESH,
        )

    pl.semaphore_wait(line_sem, len(relays))

    @pl.when(c == 1)
    def _():
        for dz in z_offsets:
            z_copy(dz).start()
        m_first()

    def d_copy(d):
        at = pl.ds(pl.multiple_of(fs * rk, rk), rk)
        return pltpu.make_async_remote_copy(
            dall.at[:, at], dall.at[:, at], d_send, d_recv, device_id=fs_peer(d), device_id_type=MESH
        )

    back_copies = (
        pltpu.make_async_remote_copy(
            fx.at[0], fx.at[0], back_sem.at[0], back_sem.at[1], device_id=partner, device_id_type=MESH
        ),
        pltpu.make_async_remote_copy(
            dall, dall, back_sem.at[2], back_sem.at[3], device_id=partner, device_id_type=MESH
        ),
    )

    def m_onward():
        arrived(masters.at[:, :, pl.ds(0, len(axis_offsets) * rows)], mf_recv)
        for k in range(1, NX):
            for j in y_offsets:
                m_copy(0, fs_source(k), md_send, md_recv, fs_peer(j * NX)).start()
        for k in range(1, NY):
            for j in x_offsets:
                m_copy(1, fs_source(k * NX), md_send, md_recv, fs_peer(j)).start()

    pl.when(c == 0)(m_onward)

    @pl.when(c == 1)
    def _():
        for copy in moment_copies:
            copy.wait_recv()
        arrived(zb.at[pl.ds(1, NZ - 1)], z_recv)
        wholes = [psf[m, :, :, pl.ds(pl.multiple_of(z * width, width), width)] for m in range(2)]
        for dz in range(1, NZ):
            for m in range(2):
                wholes[m] = wholes[m] + zb[dz, m].astype(F32)
        updated = []
        for m in range(2):
            part = wholes[m].reshape(rk, width)
            first_in = jnp.concatenate([fm[0, :, m, :], fm[1, :, m, :]], axis=1)
            second_in = jnp.concatenate([sm[0, :, m, :], sm[1, :, m, :]], axis=1)
            first = BETA_FIRST * first_in + (1.0 - BETA_FIRST) * part
            second = BETA_SECOND * second_in + (1.0 - BETA_SECOND) * part * part
            dall[m, pl.ds(pl.multiple_of(fs * rk, rk), rk), :] = (first / jnp.sqrt(second)).astype(BF16)
            updated.append((first, second))
        for d in fs_offsets:
            d_copy(d).start()
        for m in range(2):
            for k in range(2):
                for i in range(2):
                    fx[i, k, :, m, :] = updated[m][k][:, i * half : (i + 1) * half]
        back_copies[0].start()

    pl.when(c == 1)(m_onward)

    def c_copy(dz, core):
        return pltpu.make_async_remote_copy(
            cb.at[0],
            cb.at[dz],
            c_send,
            c_recv,
            device_id=(y, x, lax.rem(z + dz, NZ), core),
            device_id_type=MESH,
        )

    @pl.when(c == 1)
    def _():
        arrived(dall.at[:, pl.ds(0, (NFS - 1) * rk)], d_recv)
        for m in range(2):
            wide = dall[m].astype(F32)
            cb[0, pl.ds(m, 1), :] = jnp.sum(wide * wide, axis=0, keepdims=True)
        for dz in z_offsets:
            for core in range(2):
                c_copy(dz, core).start()
        c_copy(0, 0).start()
        back_copies[1].start()

    pl.when(c == 0)(lambda: back_copies[1].wait_recv())

    po_copy.wait_recv()
    for m in range(2):
        turned = lax.dot_general(
            dall[m], order, (((0,), (0,)), ((), ())), preferred_element_type=F32
        ).astype(BF16)
        raws[m] = jnp.dot(
            jnp.where(c == 0, turned[:half], turned[half:]),
            pboth[m].reshape(rank, pboth.shape[-1]),
            preferred_element_type=F32,
        )

    pl.when(c == 0)(lambda: arrived(cb.at[pl.ds(0, NZ)], c_recv))
    pl.when(c == 1)(lambda: arrived(cb.at[pl.ds(1, NZ - 1)], c_recv))
    squares = cb[0]
    for dz in range(1, NZ):
        squares = squares + cb[dz]
    clip_level = CLIP_SHARE * math.sqrt(rank * width * NZ)
    factors = []
    for m in range(2):
        norm = jnp.sqrt(jnp.sum(squares[m : m + 1], axis=(0, 1), keepdims=True))
        factors.append(clip_level / jnp.maximum(norm, clip_level))
    steps = (sg_out, so_out)
    news = (gn_out, on_out)
    for m in range(2):
        step = raws[m, :, own_lanes] * factors[m]
        steps[m][...] = step
        news[m][...] = masters[m, :, own_lanes] - LEARN_RATE * step
    diagonal = (NY - 1) * (NX - 1)
    arrived(masters.at[:, :, pl.ds(0, diagonal * rows)], md_recv)
    for m in range(2):
        ebuf[m] = (masters[m] - LEARN_RATE * (raws[m] * factors[m])).astype(BF16)

    for h in range(2):
        arrived(pfull.at[h, :, pl.ds(0, (NFS - 1) * rows)], p_send.at[h])
    po_copy.wait_send()
    arrived(masters.at[:, :, pl.ds(0, len(axis_offsets) * rows)], mf_send)
    arrived(masters.at[:, :, pl.ds(0, diagonal * rows)], md_send)

    @pl.when(c == 0)
    def _():
        for h in range(2):
            arrived(rs.at[0, h], rs_send.at[h])
        for copy in moment_copies:
            copy.wait_send()
        back_copies[0].wait_recv()

    @pl.when(c == 1)
    def _():
        for h in range(2):
            arrived(rs.at[0, h, pl.ds(0, NFS - 1)], rs_send.at[h])
        arrived(zb.at[pl.ds(0, NZ - 1)], z_send)
        arrived(dall.at[:, pl.ds(0, (NFS - 1) * rk)], d_send)
        arrived(cb.at[pl.ds(0, 2 * NZ - 1)], c_send)
        for copy in back_copies:
            copy.wait_send()

    fn_out[...] = fx[c, 0]
    sn_out[...] = fx[c, 1]
    for copy in swaps(x_hbm, g_hbm):
        copy.wait_send()


def store_kernel(*refs):
    count = (len(refs) - 2) // 2
    ins, outs, sem = refs[:count], refs[count:-1], refs[-1]
    sources = [*ins[:-1], ins[-1].at[0], ins[-1].at[1]]
    copies = [pltpu.make_async_copy(src, dst, sem.at[i]) for i, (src, dst) in enumerate(zip(sources, outs))]
    for copy in copies:
        copy.start()
    for copy in copies:
        copy.wait()


def shards(sizes, x, g, cv, b, proj, fm, sm, gm, om):
    NY, NX, NZ = sizes
    NFS = NY * NX
    tokens, d_model = x.shape
    channels = g.shape[1]
    rows, _, rank = proj.shape
    rk = rank // NFS
    cols = gm.shape[1]
    width = 2 * cols
    vmem = pl.BlockSpec(memory_space=pltpu.VMEM)
    hbm = pl.BlockSpec(memory_space=pltpu.HBM)
    dma = pltpu.SemaphoreType.DMA
    small = jax.ShapeDtypeStruct(fm.shape, F32)
    block = jax.ShapeDtypeStruct((cols, rows), F32)
    copy = jax.ShapeDtypeStruct((cols, d_model), BF16)
    results = pl.pallas_call(
        functools.partial(kernel, sizes),
        out_shape=(small, small, block, block, block, block, jax.ShapeDtypeStruct((2, cols, d_model), BF16)),
        in_specs=[hbm] * 9,
        out_specs=(vmem,) * 7,
        scratch_shapes=[
            pltpu.VMEM(proj.shape, BF16),
            pltpu.VMEM((2, *fm.shape), F32),
            pltpu.VMEM((2, *sm.shape), F32),
            pltpu.VMEM((2, tokens, d_model), BF16),
            pltpu.VMEM((2, tokens, channels), BF16),
            pltpu.VMEM((2, 2, rank // 2, d_model), BF16),
            pltpu.VMEM((2, cols, d_model), F32),
            pltpu.VMEM((2, cols, d_model), F32),
            pltpu.VMEM((2, rank // 2, 2 * tokens), F32),
            pltpu.VMEM((2, NFS, rk // 2, channels), F32),
            pltpu.VMEM((2, NFS, rk // 2, channels), BF16),
            pltpu.VMEM((2, 2, NFS, rk // 2, channels), BF16),
            pltpu.VMEM((2, 2, rk // 2, channels), F32),
            pltpu.VMEM((2, 2, rk // 2, channels), BF16),
            pltpu.VMEM((NZ, 2, 2, rk // 2, width), BF16),
            pltpu.VMEM((2, rank, width), BF16),
            pltpu.VMEM((2 * NZ, 2, width), F32),
            pltpu.VMEM((2, 2, *fm.shape), F32),
            dma((7,)),
            dma((2,)),
            dma((2,)),
        ]
        + [dma((2,)), dma((2, NX + NY - 2)), dma((2, NY))]
        + [dma((2,)), dma((2, 2))]
        + [dma] * 6
        + [dma((2,))]
        + [dma] * 4
        + [pltpu.SemaphoreType.REGULAR]
        + [dma((2,)), dma((2,)), dma((4,))],
        compiler_params=pltpu.CompilerParams(collective_id=0, has_side_effects=True, vmem_limit_bytes=48 * 2**20),
    )(*(pltpu.with_memory_space_constraint(a, pltpu.HBM) for a in (x, g, cv, b, proj, fm, sm, gm.T, om)))
    fn, sn, sg, so, gn, on, gc, oc = pl.pallas_call(
        store_kernel,
        out_shape=(small, small, block, block, block, block, copy, copy),
        in_specs=[vmem] * 7,
        out_specs=(hbm,) * 8,
        scratch_shapes=[dma((8,))],
        compiler_params=pltpu.CompilerParams(vmem_limit_bytes=2**20),
    )(*results)
    return fn, sn, sg.T, so, gn.T, on, gc.T, oc


def solution(mesh):
    sizes = (4, 4, 8)
    split = Mesh(mesh.devices.reshape(*sizes, 2), FS_TP)
    return build(split, sizes)


def build(split, sizes):
    in_specs = (
        P(FS_TP, None),
        P(FS_TP, None),
        P(FS_TP, None),
        P(FS_TP, None),
        P(FS, None, None),
        P(FS, None, TP),
        P(FS, None, TP),
        P(FS, TP),
        P(TP, FS),
    )
    out_specs = (
        P(FS, None, TP),
        P(FS, None, TP),
        P(FS, TP),
        P(TP, FS),
        P(FS, TP),
        P(TP, FS),
        P(None, TP),
        P(TP, None),
    )
    return jax.shard_map(
        functools.partial(shards, sizes), mesh=split, in_specs=in_specs, out_specs=out_specs, check_vma=False
    )
```
